256 devices in a mesh: ep: 64 (over z, x, core), tp: 4 (over y).
Axes of the slice: x: 4, y: 4, z: 8, core: 2. Of those that a mesh axis runs over, the one named last changes fastest.
Arguments:
- queries: bfloat16 [32768, 1024], P('ep', 'tp'), may hold values from -6 to 6
- forget_forward_logits: bfloat16 [32768, 1024], P('ep', 'tp'), may hold values from -6 to 12
- forget_backward_logits: bfloat16 [32768, 1024], P('ep', 'tp'), may hold values from -6 to 12
- values: bfloat16 [32768, 1024], P('ep', 'tp'), may hold values from -6 to 6
- output_gate_logits: bfloat16 [32768, 1024], P('ep', 'tp'), may hold values from -6 to 6
- lower_bound_forward: float32 [1024], P('tp')
- lower_bound_backward: float32 [1024], P('tp')
- extra_log_decay: float32 [32768, 8], P('ep', 'tp'), may hold values from -2 to 0
- head_norm_scale: float32 [1024], P('tp'), may hold values from 0.1 to 1.9
- output_projection: bfloat16 [1024, 2048], P('tp'), may hold values from -0.1875 to 0.1875
- second_residual: bfloat16 [32768, 2048], P('ep'), may hold values from -6 to 6
- expert_norm_scale: float32 [2048], replicated, may hold values from 0.1 to 1.9
- routes: int32 [32768, 2], P('ep'), may hold values from 0 to 63, all different within a row; in each aligned block of 128 rows (0 to 127, 128 to 255, ...) at most 8 rows name the same one
- specialist_mixing_factor: float32 [32768, 2], P(('ep', 'tp')), may hold values from 0.1 to 1
- expert_gate_matrix: bfloat16 [64, 2048, 1024], P('ep', None, 'tp'), may hold values from -0.125 to 0.125
- expert_up_matrix: bfloat16 [64, 2048, 1024], P('ep', None, 'tp'), may hold values from -0.125 to 0.125
- expert_down_matrix: bfloat16 [64, 1024, 2048], P('ep', 'tp'), may hold values from -0.1875 to 0.1875
Outputs:
- mixer_output: bfloat16 [32768, 2048], P(('ep', 'tp'))
- routed_output: bfloat16 [32768, 2048], P(('ep', 'tp'))
The draws below stay inside these ranges and needn't reach their ends.
Inputs may be any that keep to these rules, and one draw needn't show every extreme that they name: `routes`: in each aligned block of 128 rows no expert is named by more than 8 rows; the 2 experts of a row differ.
All inputs are finite; a program needn't handle non-finite values.
Results may differ from the reference program's by a relative error of at most 0.014.
Values may be sent and summed in bfloat16 or wider, within the bound.
A program may use at most 128 MiB of HBM per device.

```python
import math
import jax
import jax.numpy as jnp
import numpy as np
from jax import lax

D = 2048
RECURRENT_HEADS = 8
DK = 128
DV = 128
FF = 1024
TOPK = 2
SPAN = 64
ROWS = 128
KEY_WIDTH = 1024
VAL_WIDTH = 1024
GROUP_WIDTH = 256
EXPERT_PART = 256
EXPERTS = 64
CAPQ = 8
TOKENS_A = 32768
TOKENS_B = 32768
N_EP = 64
N_TP = 4


def floor_common(key, salt):
    key = jax.random.fold_in(key, salt)
    key_order, key_slow, key_fast = jax.random.split(key, 3)
    ordering = jax.random.permutation(key_order, RECURRENT_HEADS)
    slow_heads = ordering < RECURRENT_HEADS // 2
    slow_rate = jax.random.uniform(key_slow, (RECURRENT_HEADS, DK), jnp.float32, 0.3, 2.0) / TOKENS_A
    fast_rate = jnp.exp(jax.random.uniform(key_fast, (RECURRENT_HEADS, DK), jnp.float32, math.log(0.025), math.log(0.1)))
    decay_rate = jnp.where(slow_heads[:, None], slow_rate, fast_rate)
    return (jnp.log1p(-decay_rate) - jnp.log(decay_rate)).reshape(RECURRENT_HEADS * DK).astype(jnp.float32)


def draw_lower_bound_forward(key, part):
    return floor_common(key, 11)


def draw_lower_bound_backward(key, part):
    return floor_common(key, 12)


def forget_common(key, salt):
    key = jax.random.fold_in(key, salt)
    key_base, key_run = jax.random.split(key, 2)
    base = jnp.clip(1.5 * jax.random.normal(key_base, (TOKENS_A, RECURRENT_HEADS, DK), jnp.float32), -6.0, 6.0)
    run_length = 4 * SPAN
    run_count = (TOKENS_A + run_length - 1) // run_length
    lifted = 6.0 * jax.random.randint(key_run, (run_count, RECURRENT_HEADS), 0, 2).astype(jnp.float32)
    position_block = jnp.arange(TOKENS_A, dtype=jnp.int32) // run_length
    offsets = lifted[position_block]
    return (base + offsets[:, :, None]).reshape(TOKENS_A, RECURRENT_HEADS * DK).astype(jnp.float32)


def draw_forget_forward_logits(key, part):
    return forget_common(key, 21).astype(jnp.bfloat16)


def draw_forget_backward_logits(key, part):
    return forget_common(key, 22).astype(jnp.bfloat16)


def draw_extra_log_decay(key, part):
    key_rate, key_place, key_depth = jax.random.split(key, 3)
    span_rows = TOKENS_A // EXPERTS
    factor = jnp.exp(jax.random.uniform(key_rate, (EXPERTS, RECURRENT_HEADS), jnp.float32, 0.0, math.log(3.0)))
    token_position = jnp.arange(TOKENS_A, dtype=jnp.int32)
    owner_block = token_position // span_rows
    stable_state = -0.2 / TOKENS_A * factor[owner_block]
    slot_positions = jax.random.randint(key_place, (2, RECURRENT_HEADS), 0, TOKENS_A)
    cumulative_decay = jnp.log(jax.random.uniform(key_depth, (2, RECURRENT_HEADS), jnp.float32, 0.55, 0.8))
    extra_decay_hits = token_position[:, None, None] == slot_positions[None, :, :]
    return (stable_state + jnp.sum(jnp.where(extra_decay_hits, cumulative_decay[None], 0.0), axis=1)).astype(jnp.float32)


def shard_levels(key, shape, cuts, low, high):
    level, own = 1.0, jax.random.fold_in(key, 6)
    for position, shards_of in cuts:
        draws = jnp.exp(jax.random.uniform(jax.random.fold_in(own, position), (shards_of,), jnp.float32, low / len(cuts), high / len(cuts)))
        level = level * jnp.repeat(draws, shape[position] // shards_of).reshape([-1 if axis == position else 1 for axis in range(len(shape))])
    return level


def deal_out(own_key, own, number, rows, count, top, most, lean):
    ranking = jax.random.permutation(own_key, count)
    crowded, common = load_shares(count, rows * top, most, lean, True), load_shares(count, rows * top, most, lean, False)
    places = jnp.arange(count)

    def named(sizes, offset_by):
        used = int((sizes > 0).sum())
        fixed = max(1, used // 4)
        passed = fixed + (places - fixed + offset_by * (used - fixed)) % max(1, count - fixed)
        return jnp.zeros((count,), jnp.int32).at[ranking[jnp.where(places < fixed, places, passed)]].set(jnp.asarray(sizes, jnp.int32))

    sizes = jnp.where(number % 4 == 0, named(crowded, number // 4), named(common, number - number // 4 - 1))
    mixed = jax.random.permutation(jax.random.fold_in(own, 3), count)
    source_of, receiver = mixed[0:count // 2 * 2:2], mixed[1:count // 2 * 2:2]
    slack = jnp.minimum(sizes[source_of] - 1, most - sizes[receiver]) // 2
    slack = jnp.where((source_of == ranking[0]) | (receiver == ranking[0]) | (sizes[receiver] == 0), 0, jnp.maximum(slack, 0))
    passed = jax.random.randint(jax.random.fold_in(own, 4), (count // 2,), 0, 1 << 20) % (slack + 1)
    sizes = sizes.at[source_of].add(-passed).at[receiver].add(passed)
    members = jnp.searchsorted(jnp.cumsum(sizes), jnp.arange(rows * top), side="right").astype(jnp.int32)
    table = members.reshape(top, rows).T
    table = table[jax.random.permutation(jax.random.fold_in(own, 1), rows)]
    offset_by = jax.random.randint(jax.random.fold_in(own, 2), (rows, 1), 0, top)
    return jnp.take_along_axis(table, (jnp.arange(top)[None, :] + offset_by) % top, axis=1)


def load_shares(count, total, bound, skew, full):
    weights = [(1 << 20) // math.isqrt(standing ** skew) + 1 for standing in range(1, count + 1)]
    largest = bound if full else min(bound, max(-(-total // count), total * weights[0] // sum(weights)))
    least = 1 if total - largest >= count - 1 else 0
    given, rest = [largest] + [least] * (count - 1), total - largest - least * (count - 1)
    while rest > 0:
        movable = [i for i in range(1, count) if given[i] < largest] or [i for i in range(1, count) if given[i] < bound]
        mass, remaining = sum([weights[i] for i in movable]), rest
        for i in movable:
            extra = min(bound - given[i], max(1, remaining * weights[i] // mass), rest)
            given[i] = given[i] + extra
            rest = rest - extra
    return np.array(given)


def noise(stream_key, shape, deviation, bound, shards=(), held_as=jnp.bfloat16):
    loudness = shard_levels(stream_key, shape, shards, -0.22, 0.18) if shards else 1.0
    entries = jax.random.normal(stream_key, shape, jnp.float32) * deviation * loudness
    return jnp.minimum(jnp.maximum(entries, -bound), bound).astype(held_as)


def setup_inputs(seed: int = 0) -> dict:
    arg_keys = jax.random.split(jax.random.key(seed), 18)
    queries = noise(arg_keys[0], (TOKENS_A, KEY_WIDTH), 1.0, 6.0, ((0, 64), (1, 4)))
    forget_forward_logits = draw_forget_forward_logits(jax.random.fold_in(arg_keys[17], 71), 0)
    forget_backward_logits = draw_forget_backward_logits(jax.random.fold_in(arg_keys[17], 71), 0)
    values = noise(arg_keys[3], (TOKENS_A, VAL_WIDTH), 1.0, 6.0, ((0, 64), (1, 4)))
    output_gate_logits = noise(arg_keys[4], (TOKENS_A, VAL_WIDTH), 1.0, 6.0, ((0, 64), (1, 4)))
    lower_bound_forward = draw_lower_bound_forward(jax.random.fold_in(arg_keys[17], 71), 0)
    lower_bound_backward = draw_lower_bound_backward(jax.random.fold_in(arg_keys[17], 71), 0)
    extra_log_decay = draw_extra_log_decay(jax.random.fold_in(arg_keys[17], 71), 0)
    head_norm_scale = jnp.clip(1.0 + 0.18 * jax.random.normal(arg_keys[8], (VAL_WIDTH,), jnp.float32), 0.1, 1.9)
    output_projection = noise(arg_keys[9], (VAL_WIDTH, D), VAL_WIDTH ** -0.5, 0.1875, ((0, 4),))
    second_residual = noise(arg_keys[10], (TOKENS_B, D), 1.0, 6.0, ((0, 64),))
    expert_norm_scale = jnp.clip(1.0 + 0.18 * jax.random.normal(arg_keys[11], (D,), jnp.float32), 0.1, 1.9)
    routes_keys = jax.random.split(jax.random.fold_in(arg_keys[12], 1), TOKENS_B // ROWS)
    routes_turns = jax.random.permutation(jax.random.fold_in(arg_keys[12], 3), TOKENS_B // ROWS)
    routes = jax.vmap(lambda own, number: deal_out(jax.random.fold_in(arg_keys[12], 2), own, number, ROWS, EXPERTS, TOPK, CAPQ, 2))(routes_keys, routes_turns).reshape((TOKENS_B, TOPK))
    specialist_mixing_factor = jnp.clip(0.1 + 0.9 * jax.random.uniform(arg_keys[13], (TOKENS_B, TOPK), jnp.float32) ** shard_levels(arg_keys[13], (TOKENS_B, TOPK), ((0, 256),), -0.2, 0.2), 0.1, 1.0)
    expert_gate_matrix = noise(arg_keys[14], (EXPERTS, D, FF), D ** -0.5, 0.125, ((0, 64), (2, 4)))
    expert_up_matrix = noise(arg_keys[15], (EXPERTS, D, FF), D ** -0.5, 0.125, ((0, 64), (2, 4)))
    expert_down_matrix = noise(arg_keys[16], (EXPERTS, FF, D), FF ** -0.5, 0.1875, ((0, 64), (1, 4)))
    return dict(queries=queries, forget_forward_logits=forget_forward_logits, forget_backward_logits=forget_backward_logits, values=values, output_gate_logits=output_gate_logits, lower_bound_forward=lower_bound_forward, lower_bound_backward=lower_bound_backward, extra_log_decay=extra_log_decay, head_norm_scale=head_norm_scale, output_projection=output_projection, second_residual=second_residual, expert_norm_scale=expert_norm_scale, routes=routes, specialist_mixing_factor=specialist_mixing_factor, expert_gate_matrix=expert_gate_matrix, expert_up_matrix=expert_up_matrix, expert_down_matrix=expert_down_matrix)


EPS = 1e-06
PRECISE_PRODUCT = lax.Precision.HIGHEST

def block_pass(feature, key_matrix_rows, value_rows, log_forget_decay):
    row_count, number_of_heads, channels = feature.shape
    blocks = row_count // SPAN
    lower_mask = jnp.tril(jnp.ones((SPAN, SPAN), bool))[:, :, None, None]

    def shaped(tensor):
        return tensor.reshape(blocks, SPAN, number_of_heads, tensor.shape[-1])

    def advance(progress, inputs):
        recurrent_memory, offset = progress
        query_tile_rows, address_piece_entries, content_piece_entries, decay_block = inputs
        progressive_summary = jnp.cumsum(decay_block, axis=0)
        spread_log = jnp.where(lower_mask, progressive_summary[:, None] - progressive_summary[None, :], -jnp.inf)
        scores = lax.optimization_barrier(jnp.sum(query_tile_rows[:, None] * address_piece_entries[None, :] * jnp.exp(spread_log), axis=-1))
        inner_part = jnp.einsum('tsh,shv->thv', scores, content_piece_entries, precision=PRECISE_PRODUCT)
        handed_summary = jnp.einsum('wbf,bfl->wbl', query_tile_rows * jnp.exp(progressive_summary), recurrent_memory, precision=PRECISE_PRODUCT)
        segment_fading_total = progressive_summary[-1]
        trained_portion = jnp.einsum('gkf,gkr->kfr', address_piece_entries * jnp.exp(segment_fading_total[None] - progressive_summary), content_piece_entries, precision=PRECISE_PRODUCT)
        recurrent_memory = jnp.exp(segment_fading_total)[:, :, None] * recurrent_memory + trained_portion
        return ((recurrent_memory, offset + segment_fading_total), (inner_part + handed_summary, query_tile_rows * jnp.exp(progressive_summary + offset)))
    initial = (jnp.zeros((number_of_heads, channels, value_rows.shape[-1]), jnp.float32), jnp.zeros((number_of_heads, channels), jnp.float32))
    (recurrent_memory, decay_total), (output_rows, query_decay_reach) = lax.scan(advance, initial, (shaped(feature), shaped(key_matrix_rows), shaped(value_rows), shaped(log_forget_decay)))
    return (output_rows.reshape(row_count, number_of_heads, -1), query_decay_reach.reshape(row_count, number_of_heads, channels), recurrent_memory, decay_total)

def forget_gate_terms(forget_gate_input, lower_bound_logit, extra_decay_rows, number_of_heads):
    row_count = forget_gate_input.shape[0]
    widened_values = forget_gate_input.astype(jnp.float32).reshape(row_count, number_of_heads, -1)
    lower_bound_share = jax.nn.sigmoid(lower_bound_logit).reshape(number_of_heads, -1)
    remaining_fraction = jax.nn.sigmoid(-lower_bound_logit).reshape(number_of_heads, -1)
    log_forget_decay = jnp.log(lower_bound_share + remaining_fraction * jax.nn.sigmoid(widened_values)) + extra_decay_rows[:, :, None]
    return (remaining_fraction * jax.nn.sigmoid(-widened_values), log_forget_decay)

def finish_heads(combined, head_norm_scale, output_gate_logits, number_of_heads):
    mean_square = lax.optimization_barrier(jnp.mean(combined * combined, axis=-1, keepdims=True))
    scaled = combined * lax.rsqrt(mean_square + EPS) * head_norm_scale.reshape(number_of_heads, -1)
    opened = scaled * jax.nn.silu(output_gate_logits.astype(jnp.float32)).reshape(combined.shape)
    return opened.astype(jnp.bfloat16).reshape(combined.shape[0], -1)

def normalize(tensor, gain):
    widened_values = tensor.astype(jnp.float32)
    return (widened_values * lax.rsqrt(lax.optimization_barrier(jnp.mean(widened_values * widened_values, axis=-1, keepdims=True)) + EPS) * gain).astype(jnp.bfloat16)

def reference(queries, forget_forward_logits, forget_backward_logits, values, output_gate_logits, lower_bound_forward, lower_bound_backward, extra_log_decay, head_norm_scale, output_projection, second_residual, expert_norm_scale, routes, specialist_mixing_factor, expert_gate_matrix, expert_up_matrix, expert_down_matrix):
    feature = jax.nn.silu(queries.astype(jnp.float32)).reshape(TOKENS_A, RECURRENT_HEADS, DK)
    value_rows = values.astype(jnp.float32).reshape(TOKENS_A, RECURRENT_HEADS, DV)
    combined = jnp.zeros(value_rows.shape, jnp.float32)
    for forget_gate_input, lower_bound_logit, reverse in ((forget_forward_logits, lower_bound_forward, False), (forget_backward_logits, lower_bound_backward, True)):
        key_matrix_rows, log_forget_decay = forget_gate_terms(forget_gate_input, lower_bound_logit, extra_log_decay, RECURRENT_HEADS)
        if reverse:
            output_rows = block_pass(jnp.flip(feature, 0), jnp.flip(key_matrix_rows, 0), jnp.flip(value_rows, 0), jnp.flip(log_forget_decay, 0))[0]
            output_rows = jnp.flip(output_rows, 0)
        else:
            output_rows = block_pass(feature, key_matrix_rows, value_rows, log_forget_decay)[0]
        combined = combined + output_rows
    mixer_hidden = finish_heads(combined, head_norm_scale, output_gate_logits, RECURRENT_HEADS)
    summed = jnp.zeros((TOKENS_A, D), jnp.float32)
    for group_index in range(N_TP):
        lower_edge = group_index * GROUP_WIDTH
        partial_value = jnp.dot(mixer_hidden[:, lower_edge:lower_edge + GROUP_WIDTH], output_projection[lower_edge:lower_edge + GROUP_WIDTH], preferred_element_type=jnp.float32)
        summed = summed + lax.optimization_barrier(partial_value.astype(jnp.bfloat16)).astype(jnp.float32)
    mixer_output = summed.astype(jnp.bfloat16)
    routed_normed = normalize(second_residual, expert_norm_scale)
    slot_total = N_EP * N_TP * CAPQ
    token_ids = jnp.arange(TOKENS_B, dtype=jnp.int32)

    def one_expert(accumulated, expert):
        chosen = routes == expert
        weight = lax.optimization_barrier(jnp.sum(jnp.where(chosen, specialist_mixing_factor, 0.0), axis=1))
        member = jnp.any(chosen, axis=1)
        token_position = (jnp.cumsum(member.astype(jnp.int32)) - 1).astype(jnp.int32)
        token_position = jnp.where(member, token_position, slot_total).astype(jnp.int32)
        slot_table = jnp.zeros((slot_total + 1,), jnp.int32).at[token_position].set(token_ids)[:slot_total]
        slot_weight = jnp.zeros((slot_total + 1,), jnp.float32).at[token_position].set(weight)[:slot_total]
        picked = routed_normed[slot_table]
        gated = jnp.dot(picked, expert_gate_matrix[expert], preferred_element_type=jnp.float32)
        lifted = jnp.dot(picked, expert_up_matrix[expert], preferred_element_type=jnp.float32)
        expert_hidden = (jax.nn.silu(gated) * lifted).astype(jnp.bfloat16)
        down_rows = expert_down_matrix[expert]
        result = jnp.zeros((slot_total, D), jnp.float32)
        for group_index in range(N_TP):
            lower_edge = group_index * EXPERT_PART
            partial_value = jnp.dot(expert_hidden[:, lower_edge:lower_edge + EXPERT_PART], down_rows[lower_edge:lower_edge + EXPERT_PART], preferred_element_type=jnp.float32)
            result = result + lax.optimization_barrier(partial_value.astype(jnp.bfloat16)).astype(jnp.float32)
        expert_result = lax.optimization_barrier(result.astype(jnp.bfloat16)).astype(jnp.float32)
        accumulated = accumulated.at[slot_table].add(slot_weight[:, None] * expert_result)
        return (accumulated, None)
    accumulated = lax.scan(one_expert, jnp.zeros((TOKENS_B, D), jnp.float32), jnp.arange(EXPERTS, dtype=jnp.int32))[0]
    routed_output = accumulated.astype(jnp.bfloat16)
    return (mixer_output, routed_output)
```

```python
import functools

import jax
import jax.numpy as jnp
from jax import lax
from jax.experimental import pallas as pl
from jax.experimental.pallas import tpu as pltpu
from jax.sharding import Mesh
from jax.sharding import PartitionSpec as P

EP = ("ep_0", "ep_1", "ep_2")
EP_TP = ("ep_0", "ep_1", "ep_2", "tp")
EPS = 1e-06
TILE = 128
SUB = 16
CHUNKS = 4
MESH = pl.DeviceIdType.MESH
F32 = jnp.float32
BF16 = jnp.bfloat16


def dot_nt(a, b):
    return lax.dot_general(a, b, (((1,), (1,)), ((), ())), preferred_element_type=F32)


def dot_tn(a, b):
    return lax.dot_general(a, b, (((0,), (0,)), ((), ())), preferred_element_type=F32)


def dot(a, b):
    return jnp.dot(a, b, preferred_element_type=F32)


def sigmoid(x):
    return 1.0 / (1.0 + jnp.exp(-x))


def kernel(
    sizes,
    q_in,
    ff_in,
    fb_in,
    v_in,
    og_in,
    lbf_in,
    lbb_in,
    extra_in,
    hns_in,
    wo_in,
    res_in,
    ens_in,
    routes_in,
    mixw_in,
    g_in,
    u_in,
    d_in,
    mix_out,
    routed_out,
    q_v,
    ff_v,
    fb_v,
    v_v,
    og_v,
    lbf_v,
    lbb_v,
    extra_v,
    hns_v,
    wo_v,
    res_v,
    ens_v,
    routes_v,
    mixw_v,
    gu,
    dd,
    xn,
    pick,
    cwt,
    pk_send,
    arr,
    xs,
    hid,
    rt_send,
    rt_recv,
    p_s,
    k_s,
    qf,
    o_s,
    ust,
    tots,
    st_send,
    st_recv,
    inc_send,
    inc_recv,
    mh,
    mp_send,
    mp_recv,
    ld_sem,
    w_ssem,
    w_rsem,
    a_ssem,
    a_rsem,
    r_ssem,
    r_rsem,
    m_ssem,
    m_rsem,
):
    nz, nx, nc, nt = sizes
    count = nz * nx * nc
    rows = res_v.shape[0]
    width = res_v.shape[1]
    half = width // 2
    cap = pk_send.shape[1] // 2
    tokens = q_v.shape[0]
    tiles = tokens // TILE
    heads = q_v.shape[1] // TILE
    srows = st_send.shape[1] // 2
    per = TILE // srows
    ffp = gu.shape[-1]
    colc = width // CHUNKS
    halfc = colc // 2

    z, x, c = (lax.axis_index(a) for a in EP)
    t = lax.axis_index("tp")
    me = (z * nx + x) * nc + c

    def ep_id(p):
        return {
            "ep_0": lax.div(p, nx * nc),
            "ep_1": lax.rem(lax.div(p, nc), nx),
            "ep_2": lax.rem(p, nc),
            "tp": t,
        }

    def y_id(d):
        return {"ep_0": z, "ep_1": x, "ep_2": c, "tp": lax.rem(t + d, nt)}

    def peer_of(i):
        odd = lax.rem(i, 2)
        dist = odd * (count // 2 - lax.div(i + 1, 2)) - (1 - odd) * (count // 2 - lax.div(i, 2))
        return lax.rem(me + dist + count, count)

    t_rows = pl.ds(pl.multiple_of(t * rows, rows), rows)
    pairs = [
        (res_in.at[t_rows], res_v),
        (ens_in, ens_v),
        (routes_in, routes_v),
        (g_in.at[0], gu.at[0, 0]),
        (u_in.at[0], gu.at[0, 1]),
        (mixw_in, mixw_v),
        (q_in, q_v),
        (ff_in, ff_v),
        (fb_in, fb_v),
        (v_in, v_v),
        (og_in, og_v),
        (lbf_in, lbf_v),
        (lbb_in, lbb_v),
        (extra_in, extra_v),
        (hns_in, hns_v),
        (wo_in, wo_v),
    ] + [
        (d_in.at[0, :, j * colc : (j + 1) * colc], dd.at[j, 0 : d_in.shape[1]])
        for j in range(CHUNKS)
    ]
    loads = [pltpu.make_async_copy(a, b, ld_sem.at[i]) for i, (a, b) in enumerate(pairs)]
    for copy in loads:
        copy.start()

    barrier = pltpu.get_barrier_semaphore()

    @pl.loop(0, count - 1)
    def _(i):
        pl.semaphore_signal(barrier, inc=1, device_id=ep_id(peer_of(i)), device_id_type=MESH)

    for d in range(1, nt):
        pl.semaphore_signal(barrier, inc=1, device_id=y_id(d), device_id_type=MESH)

    for i in range(3):
        loads[i].wait()
    wide = res_v[...].astype(F32)
    scale = lax.rsqrt(jnp.mean(wide * wide, axis=-1, keepdims=True) + EPS)
    xn[...] = (wide * scale * ens_v[...]).astype(BF16)

    t_lanes = pl.ds(pl.multiple_of(t * rows, rows), rows)
    expert = lax.broadcasted_iota(jnp.int32, (count, rows), 0)
    hit0 = routes_v[0:1, t_lanes] == expert
    hit1 = routes_v[1:2, t_lanes] == expert
    member = jnp.where(hit0, 1.0, 0.0) + jnp.where(hit1, 1.0, 0.0)
    before = lax.broadcasted_iota(jnp.int32, (rows, rows), 0) < lax.broadcasted_iota(
        jnp.int32, (rows, rows), 1
    )
    rank = dot(member.astype(BF16), jnp.where(before, 1.0, 0.0).astype(BF16))
    slot = jnp.where(member > 0.5, rank, -1.0)
    seat = lax.broadcasted_iota(jnp.int32, (count, cap, rows), 1).astype(F32)
    chosen = jnp.where(jnp.abs(slot[:, None, :] - seat) < 0.25, 1.0, 0.0)
    pick[...] = chosen.reshape(count * cap, rows).astype(BF16)

    group = 64 // cap

    @pl.loop(0, count // group)
    def _(i):
        y = dot(pick[pl.ds(pl.multiple_of(i * 64, 64), 64), :], xn[...])
        lo = y[:, :half].reshape(group, cap, half)
        hi = y[:, half:].reshape(group, cap, half)
        pk_send[pl.ds(i * group, group)] = jnp.concatenate([lo, hi], axis=1).astype(BF16)

    for i in range(3, 5):
        loads[i].wait()
    pl.semaphore_wait(barrier, count - 1 + nt - 1)

    def y_copy(k, src, dst, d):
        return pltpu.make_async_remote_copy(
            src_ref=src,
            dst_ref=dst,
            send_sem=w_ssem.at[k],
            recv_sem=w_rsem.at[k],
            device_id=y_id(d),
            device_id_type=MESH,
        )

    g_up = y_copy(0, gu.at[0, 0], gu.at[1, 0], 1)
    u_up = y_copy(1, gu.at[0, 1], gu.at[1, 1], 1)
    u_dn = y_copy(2, gu.at[0, 1], gu.at[2, 1], nt - 1)
    g_dn = y_copy(3, gu.at[0, 0], gu.at[2, 0], nt - 1)
    g_far = y_copy(4, gu.at[1, 0], gu.at[3, 0], 1)
    u_far = y_copy(5, gu.at[2, 1], gu.at[3, 1], nt - 1)
    for copy in (g_up, u_dn, u_up, g_dn):
        copy.start()

    hh = ffp // 2

    def d_part(s, j, k):
        return dd.at[j, s * ffp + k * hh : s * ffp + (k + 1) * hh]

    def d_copies(j):
        base = 6 + 6 * j
        own = [y_copy(base + k, d_part(0, j, k), d_part(1, j, k), 1) for k in (0, 1)]
        own += [y_copy(base + 2 + k, d_part(0, j, k), d_part(2, j, k), nt - 1) for k in (1, 0)]
        far = [
            y_copy(base + 4, d_part(1, j, 0), d_part(3, j, 0), 1),
            y_copy(base + 5, d_part(2, j, 1), d_part(3, j, 1), nt - 1),
        ]
        return own, far

    d_all = [d_copies(j) for j in range(CHUNKS)]

    def exchange(src, dst, ssem, rsem):
        @pl.loop(0, count - 1)
        def _(i):
            p = peer_of(i)
            pltpu.make_async_remote_copy(
                src_ref=src.at[p],
                dst_ref=dst.at[me],
                send_sem=ssem,
                recv_sem=rsem,
                device_id=ep_id(p),
                device_id_type=MESH,
            ).start()

    def settle(ref, sem):
        part = ref.at[pl.ds(0, count - 1)]
        pltpu.make_async_copy(part, part, sem).wait()

    exchange(pk_send, arr, a_ssem.at[0], a_rsem.at[0])
    arr[me] = pk_send[me]

    for i in range(5, len(loads)):
        loads[i].wait()
    row_i = lax.broadcasted_iota(jnp.int32, (TILE, TILE), 0)
    col_i = lax.broadcasted_iota(jnp.int32, (TILE, TILE), 1)
    lower = row_i >= col_i
    upper = row_i <= col_i
    masks = (lower, upper)

    @pl.loop(0, tiles)
    def _(n):
        at = pl.ds(pl.multiple_of(n * TILE, TILE), TILE)
        for h in range(heads):
            ch = slice(h * TILE, (h + 1) * TILE)
            q = q_v[at, ch].astype(F32)
            qf[at, ch] = q * sigmoid(q)
            extra = jnp.broadcast_to(extra_v[h : h + 1, at], (TILE, TILE)).T
            for r, (f_ref, lb_ref) in enumerate(((ff_v, lbf_v), (fb_v, lbb_v))):
                key = sigmoid(-lb_ref[:, ch]) * sigmoid(-f_ref[at, ch].astype(F32))
                small = key * (
                    1.0
                    + key * (0.5 + key * ((1.0 / 3.0) + key * (0.25 + key * 0.2)))
                )
                near = key < 0.03125
                decay = jnp.where(near, -small, jnp.log(jnp.where(near, 0.5, 1.0 - key))) + extra
                tri = jnp.where(masks[r], 1.0, 0.0).astype(BF16)
                first = decay.astype(BF16)
                rest = decay - first.astype(F32)
                second = rest.astype(BF16)
                third = (rest - second.astype(F32)).astype(BF16)
                total = dot(tri, first) + (dot(tri, second) + dot(tri, third))
                p_s[r, at, ch] = total
                k_s[r, at, ch] = key
                last = total[TILE - 1 :, :] if r == 0 else total[:1, :]
                faded = (key * jnp.exp(last - total)).astype(BF16)
                ust[r * heads + h, n] = dot_tn(v_v[at, ch], faded)
                tots[r * heads + h, n] = jnp.broadcast_to(last, (8, TILE))

    for r in range(2):
        for h in range(heads):
            state = jnp.zeros((TILE, TILE), F32)
            log_total = jnp.zeros((1, TILE), F32)
            for n in range(tiles) if r == 0 else reversed(range(tiles)):
                row = tots[r * heads + h, n][:1]
                state = jnp.exp(row) * state + ust[r * heads + h, n]
                log_total = log_total + row
            message = jnp.concatenate(
                [
                    state.reshape(per, srows, TILE),
                    jnp.broadcast_to(log_total[None], (per, srows, TILE)),
                ],
                axis=1,
            )
            st_send[(r * heads + h) * per : (r * heads + h + 1) * per] = message.astype(BF16)

    exchange(st_send, st_recv, a_ssem.at[1], a_rsem.at[1])
    st_recv[me] = st_send[me]

    @pl.loop(0, tiles)
    def _(n):
        at = pl.ds(pl.multiple_of(n * TILE, TILE), TILE)
        for h in range(heads):
            ch = slice(h * TILE, (h + 1) * TILE)
            q = qf[at, ch]
            scores = None
            for r in range(2):
                total = p_s[r, at, ch]
                key = k_s[r, at, ch]
                blocks = []
                for i in range(TILE // SUB):
                    sub = slice(i * SUB, (i + 1) * SUB)
                    mid = total[i * SUB + SUB // 2 : i * SUB + SUB // 2 + 1, :]
                    q_i = (q[sub] * jnp.exp(total[sub] - mid)).astype(BF16)
                    k_i = (key * jnp.exp(jnp.minimum(mid - total, 70.0))).astype(BF16)
                    blocks.append(dot_nt(q_i, k_i))
                part = jnp.where(masks[r], jnp.concatenate(blocks, axis=0), 0.0)
                scores = part if scores is None else scores + part
            o_s[at, ch] = dot(scores.astype(BF16), v_v[at, ch])

    w0 = mixw_v[0:1, :]
    w1 = mixw_v[1:2, :]
    share = jnp.where(hit0, w0, 0.0) + jnp.where(hit1, w1, 0.0)
    weighted = chosen * share[:, None, :]
    blank = jnp.zeros_like(weighted)
    for k in range(2):
        both = jnp.concatenate([weighted, blank] if k == 0 else [blank, weighted], axis=1)
        flat = both.reshape(count * 2 * cap, rows).T
        high = flat.astype(BF16)
        cwt[0, k * rows : (k + 1) * rows] = high
        cwt[1, k * rows : (k + 1) * rows] = (flat - high.astype(F32)).astype(BF16)

    g_up.wait_recv()
    g_far.start()
    u_dn.wait_recv()
    u_far.start()
    for j in range(2):
        for copy in d_all[j][0]:
            copy.start()

    settle(arr, a_rsem.at[0])

    @pl.loop(0, count // group)
    def _(i):
        part = arr[pl.ds(i * group, group)].astype(F32)
        at = pl.ds(pl.multiple_of(i * 64, 64), 64)
        xs[at, :half] = part[:, :cap].reshape(64, half).astype(BF16)
        xs[at, half:] = part[:, cap:].reshape(64, half).astype(BF16)

    def lift(s):
        @pl.loop(0, count * cap // TILE)
        def _(i):
            at = pl.ds(pl.multiple_of(i * TILE, TILE), TILE)
            gated = dot(xs[at, :], gu[s, 0])
            lifted = dot(xs[at, :], gu[s, 1])
            hid[at, s * ffp : (s + 1) * ffp] = (gated * sigmoid(gated) * lifted).astype(BF16)

    lift(0)
    u_up.wait_recv()
    lift(1)
    g_dn.wait_recv()
    lift(2)

    settle(st_recv, a_rsem.at[1])
    side = lax.div(me * srows, heads * TILE)

    def pass_on(i, state):
        g = i + side * (count - 1 - 2 * i)
        inc_send[g] = state
        part = st_recv[g].astype(F32)
        return jnp.exp(part[srows:]) * state + part[:srows]

    lax.fori_loop(0, count, pass_on, jnp.zeros((srows, TILE), F32))
    exchange(inc_send, inc_recv, a_ssem.at[2], a_rsem.at[2])
    inc_recv[me] = inc_send[me]

    g_far.wait_recv()
    u_far.wait_recv()
    lift(3)

    def down(j):
        @pl.loop(0, count // group)
        def _(i):
            y = dot(hid[pl.ds(pl.multiple_of(i * 64, 64), 64), :], dd[j])
            lo = y[:, :halfc].reshape(group, cap, halfc)
            hi = y[:, halfc:].reshape(group, cap, halfc)
            rt_send[j, pl.ds(i * group, group)] = jnp.concatenate([lo, hi], axis=1).astype(BF16)

        exchange(rt_send.at[j], rt_recv.at[j], r_ssem.at[j], r_rsem.at[j])
        rt_recv[j, me] = rt_send[j, me]

    def finish_recurrence():
        settle(inc_recv, a_rsem.at[2])
        for r in range(2):
            for h in range(heads):
                ch = slice(h * TILE, (h + 1) * TILE)
                k = r * heads + h
                state = inc_recv[k * per : (k + 1) * per].reshape(TILE, TILE)
                for n in range(tiles) if r == 0 else reversed(range(tiles)):
                    at = slice(n * TILE, (n + 1) * TILE)
                    reach = (qf[at, ch] * jnp.exp(p_s[r, at, ch])).astype(BF16)
                    o_s[at, ch] += dot_nt(reach, state.astype(BF16))
                    state = jnp.exp(tots[k, n][:1]) * state + ust[k, n]

        @pl.loop(0, tiles)
        def _(n):
            at = pl.ds(pl.multiple_of(n * TILE, TILE), TILE)
            for h in range(heads):
                ch = slice(h * TILE, (h + 1) * TILE)
                o = o_s[at, ch]
                scaled = (
                    o
                    * lax.rsqrt(jnp.mean(o * o, axis=-1, keepdims=True) + EPS)
                    * hns_v[:, ch]
                )
                gate = og_v[at, ch].astype(F32)
                mh[at, ch] = (scaled * (gate * sigmoid(gate))).astype(BF16)

        @pl.loop(0, nt)
        def _(n):
            at = pl.ds(pl.multiple_of(n * rows, rows), rows)
            mp_send[n] = dot(mh[at, :], wo_v[...]).astype(BF16)

    for j in range(CHUNKS):
        own, far = d_all[j]
        own[0].wait_recv()
        far[0].start()
        own[2].wait_recv()
        far[1].start()
        if j + 2 < CHUNKS:
            for copy in d_all[j + 2][0]:
                copy.start()
        own[1].wait_recv()
        own[3].wait_recv()
        far[0].wait_recv()
        far[1].wait_recv()
        down(j)
        if j == 0:
            finish_recurrence()

    def mixer_copy(d):
        return pltpu.make_async_remote_copy(
            src_ref=mp_send.at[lax.rem(t + d, nt)],
            dst_ref=mp_recv.at[d - 1],
            send_sem=m_ssem.at[d - 1],
            recv_sem=m_rsem.at[d - 1],
            device_id=y_id(d),
            device_id_type=MESH,
        )

    mixers = [mixer_copy(d) for d in range(1, nt)]
    for copy in mixers:
        copy.start()

    def combine(j):
        settle(rt_recv.at[j], r_rsem.at[j])
        back = rt_recv[j].reshape(count * 2 * cap, halfc)
        y = dot(cwt[0], back) + dot(cwt[1], back)
        routed_out[:, j * colc : j * colc + halfc] = y[:rows].astype(BF16)
        routed_out[:, j * colc + halfc : (j + 1) * colc] = y[rows:].astype(BF16)

    for j in range(CHUNKS - 1):
        combine(j)
    for copy in mixers:
        copy.wait_recv()
    summed = mp_send[t].astype(F32)
    for d in range(nt - 1):
        summed = summed + mp_recv[d].astype(F32)
    mix_out[...] = summed.astype(BF16)
    combine(CHUNKS - 1)

    for copy in (g_up, u_up, u_dn, g_dn, g_far, u_far):
        copy.wait_send()
    for own, far in d_all:
        for copy in own + far:
            copy.wait_send()
    settle(pk_send, a_ssem.at[0])
    settle(st_send, a_ssem.at[1])
    settle(inc_send, a_ssem.at[2])
    for j in range(CHUNKS):
        settle(rt_send.at[j], r_ssem.at[j])
    for copy in mixers:
        copy.wait_send()


def shards(
    sizes,
    queries,
    forget_forward_logits,
    forget_backward_logits,
    values,
    output_gate_logits,
    lower_bound_forward,
    lower_bound_backward,
    extra_log_decay,
    head_norm_scale,
    output_projection,
    second_residual,
    expert_norm_scale,
    routes,
    specialist_mixing_factor,
    expert_gate_matrix,
    expert_up_matrix,
    expert_down_matrix,
):
    nz, nx, nc, nt = sizes
    count = nz * nx * nc
    tokens, width = second_residual.shape
    rows = tokens // nt
    cap = 4 * rows // count
    chan = queries.shape[1]
    heads = chan // TILE
    tiles = queries.shape[0] // TILE
    srows = 2 * heads * TILE // count
    ffp = expert_gate_matrix.shape[2]
    half = width // 2
    colc = width // CHUNKS
    operands = (
        queries,
        forget_forward_logits,
        forget_backward_logits,
        values,
        output_gate_logits,
        lower_bound_forward.reshape(1, chan),
        lower_bound_backward.reshape(1, chan),
        extra_log_decay.T,
        head_norm_scale.reshape(1, chan),
        output_projection,
        second_residual,
        expert_norm_scale.reshape(1, width),
        routes.T,
        specialist_mixing_factor.T,
        expert_gate_matrix,
        expert_up_matrix,
        expert_down_matrix,
    )
    vm = pltpu.VMEM
    scratch = [vm(a.shape, a.dtype) for a in operands[:10]]
    scratch += [vm((rows, width), BF16)]
    scratch += [vm(a.shape, a.dtype) for a in operands[11:14]]
    scratch += [
        vm((4, 2, width, ffp), BF16),
        vm((CHUNKS, 4 * ffp, colc), BF16),
        vm((rows, width), BF16),
        vm((count * cap, rows), BF16),
        vm((2, 2 * rows, count * 2 * cap), BF16),
        vm((count, 2 * cap, half), BF16),
        vm((count, 2 * cap, half), BF16),
        vm((count * cap, width), BF16),
        vm((count * cap, 4 * ffp), BF16),
        vm((CHUNKS, count, 2 * cap, colc // 2), BF16),
        vm((CHUNKS, count, 2 * cap, colc // 2), BF16),
        vm((2, tiles * TILE, chan), F32),
        vm((2, tiles * TILE, chan), F32),
        vm((tiles * TILE, chan), F32),
        vm((tiles * TILE, chan), F32),
        vm((2 * heads, tiles, TILE, TILE), F32),
        vm((2 * heads, tiles, 8, TILE), F32),
        vm((count, 2 * srows, TILE), BF16),
        vm((count, 2 * srows, TILE), BF16),
        vm((count, srows, TILE), F32),
        vm((count, srows, TILE), F32),
        vm((tiles * TILE, chan), BF16),
        vm((nt, rows, width), BF16),
        vm((nt - 1, rows, width), BF16),
        pltpu.SemaphoreType.DMA((16 + CHUNKS,)),
        pltpu.SemaphoreType.DMA((6 + 6 * CHUNKS,)),
        pltpu.SemaphoreType.DMA((6 + 6 * CHUNKS,)),
        pltpu.SemaphoreType.DMA((3,)),
        pltpu.SemaphoreType.DMA((3,)),
        pltpu.SemaphoreType.DMA((CHUNKS,)),
        pltpu.SemaphoreType.DMA((CHUNKS,)),
        pltpu.SemaphoreType.DMA((nt - 1,)),
        pltpu.SemaphoreType.DMA((nt - 1,)),
    ]
    out = jax.ShapeDtypeStruct((rows, width), BF16)
    return pl.pallas_call(
        functools.partial(kernel, sizes),
        out_shape=(out, out),
        in_specs=[pl.BlockSpec(memory_space=pl.ANY)] * len(operands),
        out_specs=(pl.BlockSpec(memory_space=pltpu.VMEM),) * 2,
        scratch_shapes=scratch,
        compiler_params=pltpu.CompilerParams(
            collective_id=0, has_side_effects=True, vmem_limit_bytes=62 * 1024 * 1024
        ),
    )(*operands)


def solution(mesh):
    tp = mesh.shape["tp"]
    ep = mesh.shape["ep"]
    sizes = (8, 4, 2, tp) if ep == 64 else (ep // 2, 1, 2, tp)
    split = Mesh(mesh.devices.reshape(sizes), EP_TP)
    return jax.shard_map(
        functools.partial(shards, sizes),
        mesh=split,
        in_specs=(
            P(EP, "tp"),
            P(EP, "tp"),
            P(EP, "tp"),
            P(EP, "tp"),
            P(EP, "tp"),
            P("tp"),
            P("tp"),
            P(EP, "tp"),
            P("tp"),
            P("tp", None),
            P(EP, None),
            P(),
            P(EP, None),
            P(EP_TP, None),
            P(EP, None, "tp"),
            P(EP, None, "tp"),
            P(EP, "tp", None),
        ),
        out_specs=(P(EP_TP, None), P(EP_TP, None)),
        check_vma=False,
    )
```

```python
import functools

import jax
import jax.numpy as jnp
from jax import lax
from jax.experimental import pallas as pl
from jax.experimental.pallas import tpu as pltpu
from jax.sharding import Mesh
from jax.sharding import PartitionSpec as P

EP = ("ep_0", "ep_1", "ep_2")
EP_TP = ("ep_0", "ep_1", "ep_2", "tp")
EPS = 1e-06
TILE = 128
SUB = 16
CHUNKS = 4
MESH = pl.DeviceIdType.MESH
F32 = jnp.float32
BF16 = jnp.bfloat16


def dot_nt(a, b):
    return lax.dot_general(a, b, (((1,), (1,)), ((), ())), preferred_element_type=F32)


def dot_tn(a, b):
    return lax.dot_general(a, b, (((0,), (0,)), ((), ())), preferred_element_type=F32)


def dot(a, b):
    return jnp.dot(a, b, preferred_element_type=F32)


def sigmoid(x):
    return 1.0 / (1.0 + jnp.exp(-x))


def kernel(
    sizes,
    q_in,
    ff_in,
    fb_in,
    v_in,
    og_in,
    lbf_in,
    lbb_in,
    extra_in,
    hns_in,
    wo_in,
    res_in,
    ens_in,
    routes_in,
    mixw_in,
    g_in,
    u_in,
    d_in,
    mix_out,
    routed_out,
    q_v,
    ff_v,
    fb_v,
    v_v,
    og_v,
    lbf_v,
    lbb_v,
    extra_v,
    hns_v,
    wo_v,
    res_v,
    ens_v,
    routes_v,
    mixw_v,
    gu,
    dd,
    xn,
    pick,
    cwt,
    pk_send,
    arr,
    xs,
    hid,
    rt_send,
    rt_recv,
    p_s,
    k_s,
    qf,
    o_s,
    ust,
    tots,
    st_send,
    st_recv,
    inc_send,
    inc_recv,
    mh,
    mp_send,
    mp_sum,
    mp_recv,
    ld_sem,
    w_ssem,
    w_rsem,
    a_ssem,
    a_rsem,
    r_ssem,
    r_rsem,
    m_ssem,
    m_rsem,
    d_rsem,
):
    nz, nx, nc, nt = sizes
    count = nz * nx * nc
    rows = res_v.shape[0]
    width = res_v.shape[1]
    half = width // 2
    cap = pk_send.shape[1] // 2
    tokens = q_v.shape[0]
    tiles = tokens // TILE
    heads = q_v.shape[1] // TILE
    srows = st_send.shape[1] // 2
    per = TILE // srows
    ffp = gu.shape[-1]
    colc = width // CHUNKS
    halfc = colc // 2

    z, x, c = (lax.axis_index(a) for a in EP)
    t = lax.axis_index("tp")
    me = (z * nx + x) * nc + c

    def ep_id(p):
        return {
            "ep_0": lax.div(p, nx * nc),
            "ep_1": lax.rem(lax.div(p, nc), nx),
            "ep_2": lax.rem(p, nc),
            "tp": t,
        }

    def y_id(d):
        return {"ep_0": z, "ep_1": x, "ep_2": c, "tp": lax.rem(t + d, nt)}

    def reach(i):
        odd = lax.rem(i, 2)
        return odd * (count // 2 - lax.div(i + 1, 2)) - (1 - odd) * (count // 2 - lax.div(i, 2))

    def peer_of(i):
        return lax.rem(me + reach(i) + count, count)

    def source_of(i):
        return lax.rem(me - reach(i) + count, count)

    t_rows = pl.ds(pl.multiple_of(t * rows, rows), rows)
    pairs = [
        (g_in.at[0], gu.at[0, 0]),
        (u_in.at[0], gu.at[0, 1]),
        (res_in.at[t_rows], res_v),
        (ens_in, ens_v),
        (routes_in, routes_v),
        (mixw_in, mixw_v),
        (q_in, q_v),
        (ff_in, ff_v),
        (fb_in, fb_v),
        (v_in, v_v),
        (og_in, og_v),
        (lbf_in, lbf_v),
        (lbb_in, lbb_v),
        (extra_in, extra_v),
        (hns_in, hns_v),
        (wo_in, wo_v),
    ]
    pairs[2:2] = [
        (d_in.at[0, :, j * colc : (j + 1) * colc], dd.at[j, 0 : d_in.shape[1]])
        for j in range(CHUNKS)
    ]
    loads = [pltpu.make_async_copy(a, b, ld_sem.at[i]) for i, (a, b) in enumerate(pairs)]
    for copy in loads:
        copy.start()

    barrier = pltpu.get_barrier_semaphore()

    for d in range(1, nt):
        pl.semaphore_signal(barrier, inc=1, device_id=y_id(d), device_id_type=MESH)

    @pl.loop(0, count - 1)
    def _(i):
        pl.semaphore_signal(barrier, inc=1, device_id=ep_id(peer_of(i)), device_id_type=MESH)

    for i in range(2 + CHUNKS):
        loads[i].wait()
    pl.semaphore_wait(barrier, count - 1 + nt - 1)

    def y_copy(k, src, dst, d):
        return pltpu.make_async_remote_copy(
            src_ref=src,
            dst_ref=dst,
            send_sem=w_ssem.at[k],
            recv_sem=w_rsem.at[k],
            device_id=y_id(d),
            device_id_type=MESH,
        )

    g_up = y_copy(0, gu.at[0, 0], gu.at[1, 0], 1)
    u_up = y_copy(1, gu.at[0, 1], gu.at[1, 1], 1)
    u_dn = y_copy(2, gu.at[0, 1], gu.at[2, 1], nt - 1)
    g_dn = y_copy(3, gu.at[0, 0], gu.at[2, 0], nt - 1)
    g_far = y_copy(4, gu.at[1, 0], gu.at[3, 0], 1)
    u_far = y_copy(5, gu.at[2, 1], gu.at[3, 1], nt - 1)
    hh = ffp // 2

    def d_part(s, j, k):
        return dd.at[j, s * ffp + k * hh : s * ffp + (k + 1) * hh]

    def d_copies(j):
        base = 6 + 6 * j
        own = [y_copy(base + k, d_part(0, j, k), d_part(1, j, k), 1) for k in (0, 1)]
        own += [y_copy(base + 2 + k, d_part(0, j, k), d_part(2, j, k), nt - 1) for k in (1, 0)]
        far = [
            y_copy(base + 4, d_part(1, j, 0), d_part(3, j, 0), 1),
            y_copy(base + 5, d_part(2, j, 1), d_part(3, j, 1), nt - 1),
        ]
        return own, far

    d_all = [d_copies(j) for j in range(CHUNKS)]

    for copy in (g_up, u_dn, u_up, g_dn):
        copy.start()
    for copy in d_all[0][0]:
        copy.start()


    for i in range(2 + CHUNKS, 5 + CHUNKS):
        loads[i].wait()
    wide = res_v[...].astype(F32)
    scale = lax.rsqrt(jnp.mean(wide * wide, axis=-1, keepdims=True) + EPS)
    xn[...] = (wide * scale * ens_v[...]).astype(BF16)

    t_lanes = pl.ds(pl.multiple_of(t * rows, rows), rows)
    expert = lax.broadcasted_iota(jnp.int32, (count, rows), 0)
    hit0 = routes_v[0:1, t_lanes] == expert
    hit1 = routes_v[1:2, t_lanes] == expert
    member = jnp.where(hit0, 1.0, 0.0) + jnp.where(hit1, 1.0, 0.0)
    before = lax.broadcasted_iota(jnp.int32, (rows, rows), 0) < lax.broadcasted_iota(
        jnp.int32, (rows, rows), 1
    )
    rank = dot(member.astype(BF16), jnp.where(before, 1.0, 0.0).astype(BF16))
    slot = jnp.where(member > 0.5, rank, -1.0)
    seat = lax.broadcasted_iota(jnp.int32, (count, cap, rows), 1).astype(F32)
    chosen = jnp.where(jnp.abs(slot[:, None, :] - seat) < 0.25, 1.0, 0.0)
    pick[...] = chosen.reshape(count * cap, rows).astype(BF16)

    group = TILE // cap
    parts = count // group

    @pl.loop(0, parts)
    def _(i):
        y = dot(pick[pl.ds(pl.multiple_of(i * TILE, TILE), TILE), :], xn[...])
        lo = y[:, :half].reshape(group, cap, half)
        hi = y[:, half:].reshape(group, cap, half)
        pk_send[pl.ds(i * group, group)] = jnp.concatenate([lo, hi], axis=1).astype(BF16)

    def exchange(src, dst, ssem, rsem):
        @pl.loop(0, count - 1)
        def _(i):
            p = peer_of(i)
            pltpu.make_async_remote_copy(
                src_ref=src.at[p],
                dst_ref=dst.at[me],
                send_sem=ssem,
                recv_sem=rsem,
                device_id=ep_id(p),
                device_id_type=MESH,
            ).start()

    def settle(ref, sem):
        part = ref.at[pl.ds(0, count - 1)]
        pltpu.make_async_copy(part, part, sem).wait()

    def dispatch(k):
        @pl.loop(k * group, min((k + 1) * group, count - 1))
        def _(i):
            p = peer_of(i)
            pltpu.make_async_remote_copy(
                src_ref=pk_send.at[p],
                dst_ref=arr.at[i],
                send_sem=a_ssem.at[0],
                recv_sem=d_rsem.at[k],
                device_id=ep_id(p),
                device_id_type=MESH,
            ).start()

    for k in range(parts // 2):
        dispatch(k)
    arr[count - 1] = pk_send[me]

    for i in range(5 + CHUNKS, len(loads)):
        loads[i].wait()
    row_i = lax.broadcasted_iota(jnp.int32, (TILE, TILE), 0)
    col_i = lax.broadcasted_iota(jnp.int32, (TILE, TILE), 1)
    lower = row_i >= col_i
    upper = row_i <= col_i
    masks = (lower, upper)

    @pl.loop(0, tiles)
    def _(n):
        at = pl.ds(pl.multiple_of(n * TILE, TILE), TILE)
        for h in range(heads):
            ch = slice(h * TILE, (h + 1) * TILE)
            q = q_v[at, ch].astype(F32)
            qf[at, ch] = q * sigmoid(q)
            extra = jnp.broadcast_to(extra_v[h : h + 1, at], (TILE, TILE)).T
            for r, (f_ref, lb_ref) in enumerate(((ff_v, lbf_v), (fb_v, lbb_v))):
                key = sigmoid(-lb_ref[:, ch]) * sigmoid(-f_ref[at, ch].astype(F32))
                small = key * (
                    1.0
                    + key * (0.5 + key * ((1.0 / 3.0) + key * (0.25 + key * 0.2)))
                )
                near = key < 0.03125
                decay = jnp.where(near, -small, jnp.log(jnp.where(near, 0.5, 1.0 - key))) + extra
                tri = jnp.where(masks[r], 1.0, 0.0).astype(BF16)
                first = decay.astype(BF16)
                rest = decay - first.astype(F32)
                second = rest.astype(BF16)
                third = (rest - second.astype(F32)).astype(BF16)
                total = dot(tri, first) + (dot(tri, second) + dot(tri, third))
                p_s[r, at, ch] = total
                k_s[r, at, ch] = key
                last = total[TILE - 1 :, :] if r == 0 else total[:1, :]
                faded = (key * jnp.exp(last - total)).astype(BF16)
                ust[r * heads + h, n] = dot_tn(v_v[at, ch], faded)
                tots[r * heads + h, n] = jnp.broadcast_to(last, (8, TILE))

    for r in range(2):
        for h in range(heads):
            state = jnp.zeros((TILE, TILE), F32)
            log_total = jnp.zeros((1, TILE), F32)
            for n in range(tiles) if r == 0 else reversed(range(tiles)):
                row = tots[r * heads + h, n][:1]
                state = jnp.exp(row) * state + ust[r * heads + h, n]
                log_total = log_total + row
            message = jnp.concatenate(
                [
                    state.reshape(per, srows, TILE),
                    jnp.broadcast_to(log_total[None], (per, srows, TILE)),
                ],
                axis=1,
            )
            st_send[(r * heads + h) * per : (r * heads + h + 1) * per] = message.astype(BF16)

    exchange(st_send, st_recv, a_ssem.at[1], a_rsem.at[1])
    st_recv[me] = st_send[me]
    for k in range(parts // 2, parts):
        dispatch(k)

    @pl.loop(0, tiles)
    def _(n):
        at = pl.ds(pl.multiple_of(n * TILE, TILE), TILE)
        for h in range(heads):
            ch = slice(h * TILE, (h + 1) * TILE)
            q = qf[at, ch]
            scores = None
            for r in range(2):
                total = p_s[r, at, ch]
                key = k_s[r, at, ch]
                blocks = []
                for i in range(TILE // SUB):
                    sub = slice(i * SUB, (i + 1) * SUB)
                    mid = total[i * SUB + SUB // 2 : i * SUB + SUB // 2 + 1, :]
                    q_i = (q[sub] * jnp.exp(total[sub] - mid)).astype(BF16)
                    k_i = (key * jnp.exp(jnp.minimum(mid - total, 70.0))).astype(BF16)
                    blocks.append(dot_nt(q_i, k_i))
                part = jnp.where(masks[r], jnp.concatenate(blocks, axis=0), 0.0)
                scores = part if scores is None else scores + part
            o_s[at, ch] = dot(scores.astype(BF16), v_v[at, ch])

    w0 = mixw_v[0:1, :]
    w1 = mixw_v[1:2, :]
    share = jnp.where(hit0, w0, 0.0) + jnp.where(hit1, w1, 0.0)
    weighted = chosen * share[:, None, :]
    blank = jnp.zeros_like(weighted)
    for k in range(2):
        both = jnp.concatenate([weighted, blank] if k == 0 else [blank, weighted], axis=1)
        flat = both.reshape(count * 2 * cap, rows).T
        high = flat.astype(BF16)
        cwt[0, k * rows : (k + 1) * rows] = high
        cwt[1, k * rows : (k + 1) * rows] = (flat - high.astype(F32)).astype(BF16)

    g_up.wait_recv()
    g_far.start()
    u_dn.wait_recv()
    u_far.start()
    settle(st_recv, a_rsem.at[1])
    side = lax.div(me * srows, heads * TILE)

    def pass_on(i, state):
        g = i + side * (count - 1 - 2 * i)
        inc_send[g] = state
        part = st_recv[g].astype(F32)
        return jnp.exp(part[srows:]) * state + part[:srows]

    lax.fori_loop(0, count, pass_on, jnp.zeros((srows, TILE), F32))
    exchange(inc_send, inc_recv, a_ssem.at[2], a_rsem.at[2])
    inc_recv[me] = inc_send[me]

    def lift(s, lo, size):
        at = pl.ds(pl.multiple_of(lo, TILE), size)
        gated = dot(xs[at, :], gu[s, 0])
        lifted = dot(xs[at, :], gu[s, 1])
        hid[at, s * ffp : (s + 1) * ffp] = (gated * sigmoid(gated) * lifted).astype(BF16)

    def lift_all(s):
        @pl.loop(0, parts // 2)
        def _(i):
            lift(s, i * (2 * TILE), 2 * TILE)

    for k in range(parts):
        landed = arr.at[pl.ds(0, min(group, count - 1 - k * group))]
        pltpu.make_async_copy(landed, landed, d_rsem.at[k]).wait()
        block = arr[k * group : (k + 1) * group].astype(F32)
        at = slice(k * TILE, (k + 1) * TILE)
        xs[at, :half] = block[:, :cap].reshape(TILE, half).astype(BF16)
        xs[at, half:] = block[:, cap:].reshape(TILE, half).astype(BF16)
        lift(0, k * TILE, TILE)

    d_all[0][0][0].wait_recv()
    d_all[0][1][0].start()
    d_all[0][0][2].wait_recv()
    d_all[0][1][1].start()
    for copy in d_all[1][0]:
        copy.start()
    u_up.wait_recv()
    lift_all(1)
    g_dn.wait_recv()
    lift_all(2)

    def finish_recurrence():
        settle(inc_recv, a_rsem.at[2])
        for r in range(2):
            for h in range(heads):
                ch = slice(h * TILE, (h + 1) * TILE)
                k = r * heads + h
                state = inc_recv[k * per : (k + 1) * per].reshape(TILE, TILE)
                for n in range(tiles) if r == 0 else reversed(range(tiles)):
                    at = slice(n * TILE, (n + 1) * TILE)
                    reach = (qf[at, ch] * jnp.exp(p_s[r, at, ch])).astype(BF16)
                    o_s[at, ch] += dot_nt(reach, state.astype(BF16))
                    state = jnp.exp(tots[k, n][:1]) * state + ust[k, n]

        @pl.loop(0, tiles)
        def _(n):
            at = pl.ds(pl.multiple_of(n * TILE, TILE), TILE)
            for h in range(heads):
                ch = slice(h * TILE, (h + 1) * TILE)
                o = o_s[at, ch]
                scaled = (
                    o
                    * lax.rsqrt(jnp.mean(o * o, axis=-1, keepdims=True) + EPS)
                    * hns_v[:, ch]
                )
                gate = og_v[at, ch].astype(F32)
                mh[at, ch] = (scaled * (gate * sigmoid(gate))).astype(BF16)

        @pl.loop(0, nt)
        def _(n):
            at = pl.ds(pl.multiple_of(n * rows, rows), rows)
            mp_send[n] = dot(mh[at, :], wo_v[...]).astype(BF16)

    finish_recurrence()

    g_far.wait_recv()
    u_far.wait_recv()
    lift_all(3)

    def down(j):
        @pl.loop(0, parts)
        def _(i):
            y = dot(hid[pl.ds(pl.multiple_of(i * TILE, TILE), TILE), :], dd[j])
            lo = y[:, :halfc].reshape(group, cap, halfc)
            hi = y[:, halfc:].reshape(group, cap, halfc)
            rt_send[j, pl.ds(i * group, group)] = jnp.concatenate([lo, hi], axis=1).astype(BF16)

        @pl.loop(0, count - 1)
        def _(i):
            p = source_of(i)
            pltpu.make_async_remote_copy(
                src_ref=rt_send.at[j, i],
                dst_ref=rt_recv.at[j, me],
                send_sem=r_ssem.at[j],
                recv_sem=r_rsem.at[j],
                device_id=ep_id(p),
                device_id_type=MESH,
            ).start()

        rt_recv[j, me] = rt_send[j, count - 1]

    hr = rows // 2

    def mixer_copy(k, src, dst, d):
        return pltpu.make_async_remote_copy(
            src_ref=src,
            dst_ref=mp_recv.at[dst],
            send_sem=m_ssem.at[k],
            recv_sem=m_rsem.at[k],
            device_id=y_id(d),
            device_id_type=MESH,
        )

    above, across, below = (lax.rem(t + d, nt) for d in (1, 2, 3))
    mix_first = [
        mixer_copy(0, mp_send.at[across, 0:hr], 0, 1),
        mixer_copy(1, mp_send.at[across, hr:rows], 1, nt - 1),
        mixer_copy(2, mp_send.at[above, hr:rows], 2, 1),
        mixer_copy(3, mp_send.at[below, 0:hr], 3, nt - 1),
    ]
    mix_second = [
        mixer_copy(4, mp_sum.at[0], 4, 1),
        mixer_copy(5, mp_sum.at[1], 5, nt - 1),
    ]

    for j in range(CHUNKS):
        own, far = d_all[j]
        if j > 0:
            own[0].wait_recv()
            far[0].start()
            own[2].wait_recv()
            far[1].start()
            for copy in d_all[j + 1][0] if j + 1 < CHUNKS else mix_first:
                copy.start()
        own[1].wait_recv()
        own[3].wait_recv()
        far[0].wait_recv()
        far[1].wait_recv()
        down(j)

    def combine(j):
        settle(rt_recv.at[j], r_rsem.at[j])
        back = rt_recv[j].reshape(count * 2 * cap, halfc)
        y = dot(cwt[0], back) + dot(cwt[1], back)
        routed_out[:, j * colc : j * colc + halfc] = y[:rows].astype(BF16)
        routed_out[:, j * colc + halfc : (j + 1) * colc] = y[rows:].astype(BF16)

    mix_first[0].wait_recv()
    mp_sum[0] = (mp_send[above, 0:hr].astype(F32) + mp_recv[0].astype(F32)).astype(BF16)
    mix_second[0].start()
    mix_first[1].wait_recv()
    mp_sum[1] = (mp_send[below, hr:rows].astype(F32) + mp_recv[1].astype(F32)).astype(BF16)
    mix_second[1].start()
    for j in range(CHUNKS - 1):
        combine(j)
    for copy in mix_first[2:] + mix_second:
        copy.wait_recv()
    for k, (one, two) in enumerate(((4, 3), (2, 5))):
        at = slice(k * hr, (k + 1) * hr)
        summed = mp_send[t, at].astype(F32) + mp_recv[one].astype(F32) + mp_recv[two].astype(F32)
        mix_out[at, :] = summed.astype(BF16)
    combine(CHUNKS - 1)

    for copy in (g_up, u_up, u_dn, g_dn, g_far, u_far):
        copy.wait_send()
    for own, far in d_all:
        for copy in own + far:
            copy.wait_send()
    settle(pk_send, a_ssem.at[0])
    settle(st_send, a_ssem.at[1])
    settle(inc_send, a_ssem.at[2])
    for j in range(CHUNKS):
        settle(rt_send.at[j], r_ssem.at[j])
    for copy in mix_first + mix_second:
        copy.wait_send()


def shards(
    sizes,
    queries,
    forget_forward_logits,
    forget_backward_logits,
    values,
    output_gate_logits,
    lower_bound_forward,
    lower_bound_backward,
    extra_log_decay,
    head_norm_scale,
    output_projection,
    second_residual,
    expert_norm_scale,
    routes,
    specialist_mixing_factor,
    expert_gate_matrix,
    expert_up_matrix,
    expert_down_matrix,
):
    nz, nx, nc, nt = sizes
    count = nz * nx * nc
    tokens, width = second_residual.shape
    rows = tokens // nt
    cap = 4 * rows // count
    chan = queries.shape[1]
    heads = chan // TILE
    tiles = queries.shape[0] // TILE
    srows = 2 * heads * TILE // count
    ffp = expert_gate_matrix.shape[2]
    half = width // 2
    colc = width // CHUNKS
    operands = (
        queries,
        forget_forward_logits,
        forget_backward_logits,
        values,
        output_gate_logits,
        lower_bound_forward.reshape(1, chan),
        lower_bound_backward.reshape(1, chan),
        extra_log_decay.T,
        head_norm_scale.reshape(1, chan),
        output_projection,
        second_residual,
        expert_norm_scale.reshape(1, width),
        routes.T,
        specialist_mixing_factor.T,
        expert_gate_matrix,
        expert_up_matrix,
        expert_down_matrix,
    )
    vm = pltpu.VMEM
    scratch = [vm(a.shape, a.dtype) for a in operands[:10]]
    scratch += [vm((rows, width), BF16)]
    scratch += [vm(a.shape, a.dtype) for a in operands[11:14]]
    scratch += [
        vm((4, 2, width, ffp), BF16),
        vm((CHUNKS, 4 * ffp, colc), BF16),
        vm((rows, width), BF16),
        vm((count * cap, rows), BF16),
        vm((2, 2 * rows, count * 2 * cap), BF16),
        vm((count, 2 * cap, half), BF16),
        vm((count, 2 * cap, half), BF16),
        vm((count * cap, width), BF16),
        vm((count * cap, 4 * ffp), BF16),
        vm((CHUNKS, count, 2 * cap, colc // 2), BF16),
        vm((CHUNKS, count, 2 * cap, colc // 2), BF16),
        vm((2, tiles * TILE, chan), F32),
        vm((2, tiles * TILE, chan), F32),
        vm((tiles * TILE, chan), F32),
        vm((tiles * TILE, chan), F32),
        vm((2 * heads, tiles, TILE, TILE), F32),
        vm((2 * heads, tiles, 8, TILE), F32),
        vm((count, 2 * srows, TILE), BF16),
        vm((count, 2 * srows, TILE), BF16),
        vm((count, srows, TILE), F32),
        vm((count, srows, TILE), F32),
        vm((tiles * TILE, chan), BF16),
        vm((nt, rows, width), BF16),
        vm((2, rows // 2, width), BF16),
        vm((6, rows // 2, width), BF16),
        pltpu.SemaphoreType.DMA((16 + CHUNKS,)),
        pltpu.SemaphoreType.DMA((6 + 6 * CHUNKS,)),
        pltpu.SemaphoreType.DMA((6 + 6 * CHUNKS,)),
        pltpu.SemaphoreType.DMA((3,)),
        pltpu.SemaphoreType.DMA((3,)),
        pltpu.SemaphoreType.DMA((CHUNKS,)),
        pltpu.SemaphoreType.DMA((CHUNKS,)),
        pltpu.SemaphoreType.DMA((6,)),
        pltpu.SemaphoreType.DMA((6,)),
        pltpu.SemaphoreType.DMA((count * cap // TILE,)),
    ]
    out = jax.ShapeDtypeStruct((rows, width), BF16)
    return pl.pallas_call(
        functools.partial(kernel, sizes),
        out_shape=(out, out),
        in_specs=[pl.BlockSpec(memory_space=pltpu.HBM)] * len(operands),
        out_specs=(pl.BlockSpec(memory_space=pltpu.VMEM),) * 2,
        scratch_shapes=scratch,
        compiler_params=pltpu.CompilerParams(
            collective_id=0, has_side_effects=True, vmem_limit_bytes=48 * 1024 * 1024
        ),
    )(*(pltpu.with_memory_space_constraint(a, pltpu.HBM) for a in operands))


def solution(mesh):
    tp = mesh.shape["tp"]
    ep = mesh.shape["ep"]
    sizes = (8, 4, 2, tp) if ep == 64 else (ep // 2, 1, 2, tp)
    split = Mesh(mesh.devices.reshape(sizes), EP_TP)
    return jax.shard_map(
        functools.partial(shards, sizes),
        mesh=split,
        in_specs=(
            P(EP, "tp"),
            P(EP, "tp"),
            P(EP, "tp"),
            P(EP, "tp"),
            P(EP, "tp"),
            P("tp"),
            P("tp"),
            P(EP, "tp"),
            P("tp"),
            P("tp", None),
            P(EP, None),
            P(),
            P(EP, None),
            P(EP_TP, None),
            P(EP, None, "tp"),
            P(EP, None, "tp"),
            P(EP, "tp", None),
        ),
        out_specs=(P(EP_TP, None), P(EP_TP, None)),
        check_vma=False,
    )
```

```python
import functools

import jax
import jax.numpy as jnp
from jax import lax
from jax.experimental import pallas as pl
from jax.experimental.pallas import tpu as pltpu
from jax.sharding import Mesh
from jax.sharding import PartitionSpec as P

EP = ("ep_0", "ep_1", "ep_2")
EP_TP = ("ep_0", "ep_1", "ep_2", "tp")
EPS = 1e-06
TILE = 128
SUB = 16
CHUNKS = 4
MESH = pl.DeviceIdType.MESH
F32 = jnp.float32
BF16 = jnp.bfloat16


def dot_nt(a, b):
    return lax.dot_general(a, b, (((1,), (1,)), ((), ())), preferred_element_type=F32)


def dot_tn(a, b):
    return lax.dot_general(a, b, (((0,), (0,)), ((), ())), preferred_element_type=F32)


def dot(a, b):
    return jnp.dot(a, b, preferred_element_type=F32)


def sigmoid(x):
    return 1.0 / (1.0 + jnp.exp(-x))


def kernel(
    sizes,
    q_in,
    ff_in,
    fb_in,
    v_in,
    og_in,
    lbf_in,
    lbb_in,
    extra_in,
    hns_in,
    wo_in,
    res_in,
    ens_in,
    routes_in,
    mixw_in,
    g_in,
    u_in,
    d_in,
    mix_out,
    routed_out,
    q_v,
    ff_v,
    fb_v,
    v_v,
    og_v,
    lbf_v,
    lbb_v,
    extra_v,
    hns_v,
    wo_v,
    res_v,
    ens_v,
    routes_v,
    mixw_v,
    gu,
    dd,
    xn,
    pick,
    cwt,
    pk_send,
    arr,
    xs,
    hid,
    rt_send,
    rt_recv,
    p_s,
    k_s,
    qf,
    o_s,
    ust,
    tots,
    st_send,
    st_recv,
    inc_send,
    inc_recv,
    mh,
    mp_send,
    mp_sum,
    mp_recv,
    ld_sem,
    w_ssem,
    w_rsem,
    a_ssem,
    a_rsem,
    r_ssem,
    r_rsem,
    m_ssem,
    m_rsem,
    d_rsem,
    word_sem,
):
    nz, nx, nc, nt = sizes
    count = nz * nx * nc
    rows = res_v.shape[0]
    width = res_v.shape[1]
    half = width // 2
    cap = pk_send.shape[1] // 2
    tokens = q_v.shape[0]
    tiles = tokens // TILE
    heads = q_v.shape[1] // TILE
    srows = st_send.shape[1] // 2
    per = TILE // srows
    ffp = gu.shape[-1]
    colc = width // CHUNKS
    halfc = colc // 2

    z, x, c = (lax.axis_index(a) for a in EP)
    t = lax.axis_index("tp")
    me = (z * nx + x) * nc + c

    def ep_id(p):
        return {
            "ep_0": lax.div(p, nx * nc),
            "ep_1": lax.rem(lax.div(p, nc), nx),
            "ep_2": lax.rem(p, nc),
            "tp": t,
        }

    def y_id(d):
        return {"ep_0": z, "ep_1": x, "ep_2": c, "tp": lax.rem(t + d, nt)}

    def reach(i):
        odd = lax.rem(i, 2)
        return odd * (count // 2 - lax.div(i + 1, 2)) - (1 - odd) * (count // 2 - lax.div(i, 2))

    def peer_of(i):
        return lax.rem(me + reach(i) + count, count)

    def source_of(i):
        return lax.rem(me - reach(i) + count, count)

    t_rows = pl.ds(pl.multiple_of(t * rows, rows), rows)
    pairs = [
        (g_in.at[0], gu.at[0, 0]),
        (u_in.at[0], gu.at[0, 1]),
        (res_in.at[t_rows], res_v),
        (ens_in, ens_v),
        (routes_in, routes_v),
        (mixw_in, mixw_v),
        (q_in, q_v),
        (ff_in, ff_v),
        (fb_in, fb_v),
        (v_in, v_v),
        (og_in, og_v),
        (lbf_in, lbf_v),
        (lbb_in, lbb_v),
        (extra_in, extra_v),
        (hns_in, hns_v),
        (wo_in, wo_v),
    ]
    pairs[2:2] = [
        (d_in.at[0, :, j * colc : (j + 1) * colc], dd.at[j, 0 : d_in.shape[1]])
        for j in range(CHUNKS)
    ]
    loads = [pltpu.make_async_copy(a, b, ld_sem.at[i]) for i, (a, b) in enumerate(pairs)]
    for copy in loads:
        copy.start()

    def grid_id(dz=0, dx=0, dc=0, dy=0):
        return {
            "ep_0": lax.rem(z + dz, nz),
            "ep_1": lax.rem(x + dx, nx),
            "ep_2": lax.rem(c + dc, nc),
            "tp": lax.rem(t + dy, nt),
        }

    def greet(sem, devices):
        for device in devices:
            pl.semaphore_signal(sem, inc=1, device_id=device, device_id_type=MESH)

    line_y = [grid_id(dy=d) for d in range(1, nt)]
    plane = [grid_id(dx=i, dc=j) for i in range(nx) for j in range(nc) if i + j > 0]
    near_z = [grid_id(dz=d) for d in range(1, nz) if min(d, nz - d) <= (nz + 3) // 4]
    near = line_y + plane + near_z
    barrier = pltpu.get_barrier_semaphore()
    greet(barrier, near)

    for i in range(2 + CHUNKS):
        loads[i].wait()
    pl.semaphore_wait(barrier, len(near))

    def y_copy(k, src, dst, d):
        return pltpu.make_async_remote_copy(
            src_ref=src,
            dst_ref=dst,
            send_sem=w_ssem.at[k],
            recv_sem=w_rsem.at[k],
            device_id=y_id(d),
            device_id_type=MESH,
        )

    g_up = y_copy(0, gu.at[0, 0], gu.at[1, 0], 1)
    u_up = y_copy(1, gu.at[0, 1], gu.at[1, 1], 1)
    u_dn = y_copy(2, gu.at[0, 1], gu.at[2, 1], nt - 1)
    g_dn = y_copy(3, gu.at[0, 0], gu.at[2, 0], nt - 1)
    g_far = y_copy(4, gu.at[1, 0], gu.at[3, 0], 1)
    u_far = y_copy(5, gu.at[2, 1], gu.at[3, 1], nt - 1)
    hh = ffp // 2

    def d_part(s, j, k):
        return dd.at[j, s * ffp + k * hh : s * ffp + (k + 1) * hh]

    def d_copies(j):
        base = 6 + 6 * j
        own = [y_copy(base + k, d_part(0, j, k), d_part(1, j, k), 1) for k in (0, 1)]
        own += [y_copy(base + 2 + k, d_part(0, j, k), d_part(2, j, k), nt - 1) for k in (1, 0)]
        far = [
            y_copy(base + 4, d_part(1, j, 0), d_part(3, j, 0), 1),
            y_copy(base + 5, d_part(2, j, 1), d_part(3, j, 1), nt - 1),
        ]
        return own, far

    d_all = [d_copies(j) for j in range(CHUNKS)]

    for copy in (g_up, u_dn, u_up, g_dn):
        copy.start()
    for copy in d_all[0][0]:
        copy.start()
    greet(word_sem.at[0], near_z)


    for i in range(2 + CHUNKS, 5 + CHUNKS):
        loads[i].wait()
    wide = res_v[...].astype(F32)
    scale = lax.rsqrt(jnp.mean(wide * wide, axis=-1, keepdims=True) + EPS)
    xn[...] = (wide * scale * ens_v[...]).astype(BF16)

    pl.semaphore_wait(word_sem.at[0], len(near_z))
    greet(word_sem.at[1], plane)

    t_lanes = pl.ds(pl.multiple_of(t * rows, rows), rows)
    expert = lax.broadcasted_iota(jnp.int32, (count, rows), 0)
    hit0 = routes_v[0:1, t_lanes] == expert
    hit1 = routes_v[1:2, t_lanes] == expert
    member = jnp.where(hit0, 1.0, 0.0) + jnp.where(hit1, 1.0, 0.0)
    before = lax.broadcasted_iota(jnp.int32, (rows, rows), 0) < lax.broadcasted_iota(
        jnp.int32, (rows, rows), 1
    )
    rank = dot(member.astype(BF16), jnp.where(before, 1.0, 0.0).astype(BF16))
    slot = jnp.where(member > 0.5, rank, -1.0)
    seat = lax.broadcasted_iota(jnp.int32, (count, cap, rows), 1).astype(F32)
    chosen = jnp.where(jnp.abs(slot[:, None, :] - seat) < 0.25, 1.0, 0.0)
    pick[...] = chosen.reshape(count * cap, rows).astype(BF16)

    group = TILE // cap
    parts = count // group

    @pl.loop(0, parts)
    def _(i):
        y = dot(pick[pl.ds(pl.multiple_of(i * TILE, TILE), TILE), :], xn[...])
        lo = y[:, :half].reshape(group, cap, half)
        hi = y[:, half:].reshape(group, cap, half)
        pk_send[pl.ds(i * group, group)] = jnp.concatenate([lo, hi], axis=1).astype(BF16)

    def exchange(src, dst, ssem, rsem):
        @pl.loop(0, count - 1)
        def _(i):
            p = peer_of(i)
            pltpu.make_async_remote_copy(
                src_ref=src.at[p],
                dst_ref=dst.at[me],
                send_sem=ssem,
                recv_sem=rsem,
                device_id=ep_id(p),
                device_id_type=MESH,
            ).start()

    def settle(ref, sem):
        part = ref.at[pl.ds(0, count - 1)]
        pltpu.make_async_copy(part, part, sem).wait()

    pl.semaphore_wait(word_sem.at[1], len(plane))

    def dispatch(k):
        @pl.loop(k * group, min((k + 1) * group, count - 1))
        def _(i):
            p = peer_of(i)
            pltpu.make_async_remote_copy(
                src_ref=pk_send.at[p],
                dst_ref=arr.at[i],
                send_sem=a_ssem.at[0],
                recv_sem=d_rsem.at[k],
                device_id=ep_id(p),
                device_id_type=MESH,
            ).start()

    for k in range(parts // 2):
        dispatch(k)
    arr[count - 1] = pk_send[me]

    for i in range(5 + CHUNKS, len(loads)):
        loads[i].wait()
    row_i = lax.broadcasted_iota(jnp.int32, (TILE, TILE), 0)
    col_i = lax.broadcasted_iota(jnp.int32, (TILE, TILE), 1)
    lower = row_i >= col_i
    upper = row_i <= col_i
    masks = (lower, upper)

    @pl.loop(0, tiles)
    def _(n):
        at = pl.ds(pl.multiple_of(n * TILE, TILE), TILE)
        for h in range(heads):
            ch = slice(h * TILE, (h + 1) * TILE)
            q = q_v[at, ch].astype(F32)
            qf[at, ch] = q * sigmoid(q)
            extra = jnp.broadcast_to(extra_v[h : h + 1, at], (TILE, TILE)).T
            for r, (f_ref, lb_ref) in enumerate(((ff_v, lbf_v), (fb_v, lbb_v))):
                key = sigmoid(-lb_ref[:, ch]) * sigmoid(-f_ref[at, ch].astype(F32))
                small = key * (
                    1.0
                    + key * (0.5 + key * ((1.0 / 3.0) + key * (0.25 + key * 0.2)))
                )
                near = key < 0.03125
                decay = jnp.where(near, -small, jnp.log(jnp.where(near, 0.5, 1.0 - key))) + extra
                tri = jnp.where(masks[r], 1.0, 0.0).astype(BF16)
                first = decay.astype(BF16)
                rest = decay - first.astype(F32)
                second = rest.astype(BF16)
                third = (rest - second.astype(F32)).astype(BF16)
                total = dot(tri, first) + (dot(tri, second) + dot(tri, third))
                p_s[r, at, ch] = total
                k_s[r, at, ch] = key
                last = total[TILE - 1 :, :] if r == 0 else total[:1, :]
                faded = (key * jnp.exp(last - total)).astype(BF16)
                ust[r * heads + h, n] = dot_tn(v_v[at, ch], faded)
                tots[r * heads + h, n] = jnp.broadcast_to(last, (8, TILE))

    for r in range(2):
        for h in range(heads):
            state = jnp.zeros((TILE, TILE), F32)
            log_total = jnp.zeros((1, TILE), F32)
            for n in range(tiles) if r == 0 else reversed(range(tiles)):
                row = tots[r * heads + h, n][:1]
                state = jnp.exp(row) * state + ust[r * heads + h, n]
                log_total = log_total + row
            message = jnp.concatenate(
                [
                    state.reshape(per, srows, TILE),
                    jnp.broadcast_to(log_total[None], (per, srows, TILE)),
                ],
                axis=1,
            )
            st_send[(r * heads + h) * per : (r * heads + h + 1) * per] = message.astype(BF16)

    exchange(st_send, st_recv, a_ssem.at[1], a_rsem.at[1])
    st_recv[me] = st_send[me]
    for k in range(parts // 2, parts):
        dispatch(k)

    @pl.loop(0, tiles)
    def _(n):
        at = pl.ds(pl.multiple_of(n * TILE, TILE), TILE)
        for h in range(heads):
            ch = slice(h * TILE, (h + 1) * TILE)
            q = qf[at, ch]
            scores = None
            for r in range(2):
                total = p_s[r, at, ch]
                key = k_s[r, at, ch]
                blocks = []
                for i in range(TILE // SUB):
                    sub = slice(i * SUB, (i + 1) * SUB)
                    mid = total[i * SUB + SUB // 2 : i * SUB + SUB // 2 + 1, :]
                    q_i = (q[sub] * jnp.exp(total[sub] - mid)).astype(BF16)
                    k_i = (key * jnp.exp(jnp.minimum(mid - total, 70.0))).astype(BF16)
                    blocks.append(dot_nt(q_i, k_i))
                part = jnp.where(masks[r], jnp.concatenate(blocks, axis=0), 0.0)
                scores = part if scores is None else scores + part
            o_s[at, ch] = dot(scores.astype(BF16), v_v[at, ch])

    w0 = mixw_v[0:1, :]
    w1 = mixw_v[1:2, :]
    share = jnp.where(hit0, w0, 0.0) + jnp.where(hit1, w1, 0.0)
    weighted = chosen * share[:, None, :]
    blank = jnp.zeros_like(weighted)
    for k in range(2):
        both = jnp.concatenate([weighted, blank] if k == 0 else [blank, weighted], axis=1)
        flat = both.reshape(count * 2 * cap, rows).T
        high = flat.astype(BF16)
        cwt[0, k * rows : (k + 1) * rows] = high
        cwt[1, k * rows : (k + 1) * rows] = (flat - high.astype(F32)).astype(BF16)

    g_up.wait_recv()
    g_far.start()
    u_dn.wait_recv()
    u_far.start()
    settle(st_recv, a_rsem.at[1])
    side = lax.div(me * srows, heads * TILE)

    def pass_on(i, state):
        g = i + side * (count - 1 - 2 * i)
        inc_send[g] = state
        part = st_recv[g].astype(F32)
        return jnp.exp(part[srows:]) * state + part[:srows]

    lax.fori_loop(0, count, pass_on, jnp.zeros((srows, TILE), F32))
    exchange(inc_send, inc_recv, a_ssem.at[2], a_rsem.at[2])
    inc_recv[me] = inc_send[me]

    def lift(s, lo, size):
        at = pl.ds(pl.multiple_of(lo, TILE), size)
        gated = dot(xs[at, :], gu[s, 0])
        lifted = dot(xs[at, :], gu[s, 1])
        hid[at, s * ffp : (s + 1) * ffp] = (gated * sigmoid(gated) * lifted).astype(BF16)

    def lift_all(s):
        @pl.loop(0, parts // 2)
        def _(i):
            lift(s, i * (2 * TILE), 2 * TILE)

    def unpack(k):
        landed = arr.at[pl.ds(0, min(group, count - 1 - k * group))]
        pltpu.make_async_copy(landed, landed, d_rsem.at[k]).wait()
        block = arr[k * group : (k + 1) * group].astype(F32)
        at = slice(k * TILE, (k + 1) * TILE)
        xs[at, :half] = block[:, :cap].reshape(TILE, half).astype(BF16)
        xs[at, half:] = block[:, cap:].reshape(TILE, half).astype(BF16)
        lift(0, k * TILE, TILE)

    for k in range(parts - 1):
        unpack(k)
    early = (parts - 1) * TILE
    u_up.wait_recv()
    g_dn.wait_recv()
    for n in (1, 2):

        @pl.loop(0, parts - 1)
        def _(i):
            lift(n, i * TILE, TILE)

    unpack(parts - 1)
    for n in (1, 2):
        lift(n, early, TILE)

    d_all[0][0][0].wait_recv()
    d_all[0][1][0].start()
    d_all[0][0][2].wait_recv()
    d_all[0][1][1].start()
    for copy in d_all[1][0]:
        copy.start()

    def finish_recurrence():
        settle(inc_recv, a_rsem.at[2])
        for r in range(2):
            for h in range(heads):
                ch = slice(h * TILE, (h + 1) * TILE)
                k = r * heads + h
                state = inc_recv[k * per : (k + 1) * per].reshape(TILE, TILE)
                for n in range(tiles) if r == 0 else reversed(range(tiles)):
                    at = slice(n * TILE, (n + 1) * TILE)
                    reach = (qf[at, ch] * jnp.exp(p_s[r, at, ch])).astype(BF16)
                    o_s[at, ch] += dot_nt(reach, state.astype(BF16))
                    state = jnp.exp(tots[k, n][:1]) * state + ust[k, n]

        @pl.loop(0, tiles)
        def _(n):
            at = pl.ds(pl.multiple_of(n * TILE, TILE), TILE)
            for h in range(heads):
                ch = slice(h * TILE, (h + 1) * TILE)
                o = o_s[at, ch]
                scaled = (
                    o
                    * lax.rsqrt(jnp.mean(o * o, axis=-1, keepdims=True) + EPS)
                    * hns_v[:, ch]
                )
                gate = og_v[at, ch].astype(F32)
                mh[at, ch] = (scaled * (gate * sigmoid(gate))).astype(BF16)

        @pl.loop(0, nt)
        def _(n):
            at = pl.ds(pl.multiple_of(n * rows, rows), rows)
            mp_send[n] = dot(mh[at, :], wo_v[...]).astype(BF16)

    finish_recurrence()

    g_far.wait_recv()
    u_far.wait_recv()
    lift_all(3)

    def down(j):
        def product(i):
            y = dot(hid[pl.ds(pl.multiple_of(i * TILE, TILE), TILE), :], dd[j])
            lo = y[:, :halfc].reshape(group, cap, halfc)
            hi = y[:, halfc:].reshape(group, cap, halfc)
            rt_send[j, pl.ds(i * group, group)] = jnp.concatenate([lo, hi], axis=1).astype(BF16)

        def give_back(first, last):
            @pl.loop(first, last)
            def _(i):
                p = source_of(i)
                pltpu.make_async_remote_copy(
                    src_ref=rt_send.at[j, i],
                    dst_ref=rt_recv.at[j, me],
                    send_sem=r_ssem.at[j],
                    recv_sem=r_rsem.at[j],
                    device_id=ep_id(p),
                    device_id_type=MESH,
                ).start()

        product(0)

        @pl.loop(1, parts)
        def _(k):
            product(k)
            give_back((k - 1) * group, k * group)

        give_back((parts - 1) * group, count - 1)
        rt_recv[j, me] = rt_send[j, count - 1]

    hr = rows // 2

    def mixer_copy(k, src, dst, d):
        return pltpu.make_async_remote_copy(
            src_ref=src,
            dst_ref=mp_recv.at[dst],
            send_sem=m_ssem.at[k],
            recv_sem=m_rsem.at[k],
            device_id=y_id(d),
            device_id_type=MESH,
        )

    above, across, below = (lax.rem(t + d, nt) for d in (1, 2, 3))
    mix_first = [
        mixer_copy(0, mp_send.at[across, 0:hr], 0, 1),
        mixer_copy(1, mp_send.at[across, hr:rows], 1, nt - 1),
        mixer_copy(2, mp_send.at[above, hr:rows], 2, 1),
        mixer_copy(3, mp_send.at[below, 0:hr], 3, nt - 1),
    ]
    mix_second = [
        mixer_copy(4, mp_sum.at[0], 4, 1),
        mixer_copy(5, mp_sum.at[1], 5, nt - 1),
    ]

    for j in range(CHUNKS):
        own, far = d_all[j]
        if j > 0:
            own[0].wait_recv()
            far[0].start()
            own[2].wait_recv()
            far[1].start()
            for copy in d_all[j + 1][0] if j + 1 < CHUNKS else mix_first:
                copy.start()
        own[1].wait_recv()
        own[3].wait_recv()
        far[0].wait_recv()
        far[1].wait_recv()
        down(j)

    def combine(j):
        settle(rt_recv.at[j], r_rsem.at[j])
        back = rt_recv[j].reshape(count * 2 * cap, halfc)
        y = dot(cwt[0], back) + dot(cwt[1], back)
        routed_out[:, j * colc : j * colc + halfc] = y[:rows].astype(BF16)
        routed_out[:, j * colc + halfc : (j + 1) * colc] = y[rows:].astype(BF16)

    mix_first[0].wait_recv()
    mp_sum[0] = (mp_send[above, 0:hr].astype(F32) + mp_recv[0].astype(F32)).astype(BF16)
    mix_second[0].start()
    mix_first[1].wait_recv()
    mp_sum[1] = (mp_send[below, hr:rows].astype(F32) + mp_recv[1].astype(F32)).astype(BF16)
    mix_second[1].start()
    for j in range(CHUNKS - 1):
        combine(j)
    for copy in mix_first[2:] + mix_second:
        copy.wait_recv()
    for k, (one, two) in enumerate(((4, 3), (2, 5))):
        at = slice(k * hr, (k + 1) * hr)
        summed = mp_send[t, at].astype(F32) + mp_recv[one].astype(F32) + mp_recv[two].astype(F32)
        mix_out[at, :] = summed.astype(BF16)
    combine(CHUNKS - 1)

    for copy in (g_up, u_up, u_dn, g_dn, g_far, u_far):
        copy.wait_send()
    for own, far in d_all:
        for copy in own + far:
            copy.wait_send()
    settle(pk_send, a_ssem.at[0])
    settle(st_send, a_ssem.at[1])
    settle(inc_send, a_ssem.at[2])
    for j in range(CHUNKS):
        settle(rt_send.at[j], r_ssem.at[j])
    for copy in mix_first + mix_second:
        copy.wait_send()


def shards(
    sizes,
    queries,
    forget_forward_logits,
    forget_backward_logits,
    values,
    output_gate_logits,
    lower_bound_forward,
    lower_bound_backward,
    extra_log_decay,
    head_norm_scale,
    output_projection,
    second_residual,
    expert_norm_scale,
    routes,
    specialist_mixing_factor,
    expert_gate_matrix,
    expert_up_matrix,
    expert_down_matrix,
):
    nz, nx, nc, nt = sizes
    count = nz * nx * nc
    tokens, width = second_residual.shape
    rows = tokens // nt
    cap = 4 * rows // count
    chan = queries.shape[1]
    heads = chan // TILE
    tiles = queries.shape[0] // TILE
    srows = 2 * heads * TILE // count
    ffp = expert_gate_matrix.shape[2]
    half = width // 2
    colc = width // CHUNKS
    operands = (
        queries,
        forget_forward_logits,
        forget_backward_logits,
        values,
        output_gate_logits,
        lower_bound_forward.reshape(1, chan),
        lower_bound_backward.reshape(1, chan),
        extra_log_decay.T,
        head_norm_scale.reshape(1, chan),
        output_projection,
        second_residual,
        expert_norm_scale.reshape(1, width),
        routes.T,
        specialist_mixing_factor.T,
        expert_gate_matrix,
        expert_up_matrix,
        expert_down_matrix,
    )
    vm = pltpu.VMEM
    scratch = [vm(a.shape, a.dtype) for a in operands[:10]]
    scratch += [vm((rows, width), BF16)]
    scratch += [vm(a.shape, a.dtype) for a in operands[11:14]]
    scratch += [
        vm((4, 2, width, ffp), BF16),
        vm((CHUNKS, 4 * ffp, colc), BF16),
        vm((rows, width), BF16),
        vm((count * cap, rows), BF16),
        vm((2, 2 * rows, count * 2 * cap), BF16),
        vm((count, 2 * cap, half), BF16),
        vm((count, 2 * cap, half), BF16),
        vm((count * cap, width), BF16),
        vm((count * cap, 4 * ffp), BF16),
        vm((CHUNKS, count, 2 * cap, colc // 2), BF16),
        vm((CHUNKS, count, 2 * cap, colc // 2), BF16),
        vm((2, tiles * TILE, chan), F32),
        vm((2, tiles * TILE, chan), F32),
        vm((tiles * TILE, chan), F32),
        vm((tiles * TILE, chan), F32),
        vm((2 * heads, tiles, TILE, TILE), F32),
        vm((2 * heads, tiles, 8, TILE), F32),
        vm((count, 2 * srows, TILE), BF16),
        vm((count, 2 * srows, TILE), BF16),
        vm((count, srows, TILE), F32),
        vm((count, srows, TILE), F32),
        vm((tiles * TILE, chan), BF16),
        vm((nt, rows, width), BF16),
        vm((2, rows // 2, width), BF16),
        vm((6, rows // 2, width), BF16),
        pltpu.SemaphoreType.DMA((16 + CHUNKS,)),
        pltpu.SemaphoreType.DMA((6 + 6 * CHUNKS,)),
        pltpu.SemaphoreType.DMA((6 + 6 * CHUNKS,)),
        pltpu.SemaphoreType.DMA((3,)),
        pltpu.SemaphoreType.DMA((3,)),
        pltpu.SemaphoreType.DMA((CHUNKS,)),
        pltpu.SemaphoreType.DMA((CHUNKS,)),
        pltpu.SemaphoreType.DMA((6,)),
        pltpu.SemaphoreType.DMA((6,)),
        pltpu.SemaphoreType.DMA((count * cap // TILE,)),
        pltpu.SemaphoreType.REGULAR((2,)),
    ]
    out = jax.ShapeDtypeStruct((rows, width), BF16)
    return pl.pallas_call(
        functools.partial(kernel, sizes),
        out_shape=(out, out),
        in_specs=[pl.BlockSpec(memory_space=pltpu.HBM)] * len(operands),
        out_specs=(pl.BlockSpec(memory_space=pltpu.VMEM),) * 2,
        scratch_shapes=scratch,
        compiler_params=pltpu.CompilerParams(
            collective_id=0, has_side_effects=True, vmem_limit_bytes=48 * 1024 * 1024
        ),
    )(*(pltpu.with_memory_space_constraint(a, pltpu.HBM) for a in operands))


def solution(mesh):
    tp = mesh.shape["tp"]
    ep = mesh.shape["ep"]
    sizes = (8, 4, 2, tp) if ep == 64 else (ep // 2, 1, 2, tp)
    split = Mesh(mesh.devices.reshape(sizes), EP_TP)
    return jax.shard_map(
        functools.partial(shards, sizes),
        mesh=split,
        in_specs=(
            P(EP, "tp"),
            P(EP, "tp"),
            P(EP, "tp"),
            P(EP, "tp"),
            P(EP, "tp"),
            P("tp"),
            P("tp"),
            P(EP, "tp"),
            P("tp"),
            P("tp", None),
            P(EP, None),
            P(),
            P(EP, None),
            P(EP_TP, None),
            P(EP, None, "tp"),
            P(EP, None, "tp"),
            P(EP, "tp", None),
        ),
        out_specs=(P(EP_TP, None), P(EP_TP, None)),
        check_vma=False,
    )
```

```python
import functools

import jax
import jax.numpy as jnp
from jax import lax
from jax.experimental import pallas as pl
from jax.experimental.pallas import tpu as pltpu
from jax.sharding import Mesh
from jax.sharding import PartitionSpec as P

EP = ("ep_0", "ep_1", "ep_2")
EP_TP = ("ep_0", "ep_1", "ep_2", "tp")
EPS = 1e-06
TILE = 128
SUB = 16
EIGHTHS = (1, 2, 2, 3)
CHUNKS = len(EIGHTHS)
MESH = pl.DeviceIdType.MESH
F32 = jnp.float32
BF16 = jnp.bfloat16


def dot_nt(a, b):
    return lax.dot_general(a, b, (((1,), (1,)), ((), ())), preferred_element_type=F32)


def dot_tn(a, b):
    return lax.dot_general(a, b, (((0,), (0,)), ((), ())), preferred_element_type=F32)


def dot(a, b):
    return jnp.dot(a, b, preferred_element_type=F32)


def sigmoid(x):
    return 1.0 / (1.0 + jnp.exp(-x))


def kernel(
    sizes,
    q_in,
    ff_in,
    fb_in,
    v_in,
    og_in,
    lbf_in,
    lbb_in,
    extra_in,
    hns_in,
    wo_in,
    res_in,
    ens_in,
    routes_in,
    mixw_in,
    g_in,
    u_in,
    d_in,
    mix_out,
    routed_out,
    q_v,
    ff_v,
    fb_v,
    v_v,
    og_v,
    lbf_v,
    lbb_v,
    extra_v,
    hns_v,
    wo_v,
    res_v,
    ens_v,
    routes_v,
    mixw_v,
    gu,
    dd0,
    dd1,
    dd2,
    dd3,
    xn,
    pick,
    cwt,
    pk_send,
    arr,
    xs,
    hid,
    rts0,
    rts1,
    rts2,
    rts3,
    rtr0,
    rtr1,
    rtr2,
    rtr3,
    p_s,
    k_s,
    qf,
    o_s,
    ust,
    tots,
    st_send,
    st_recv,
    inc_send,
    inc_recv,
    mh,
    mp_send,
    mp_sum,
    mp_recv,
    ld_sem,
    w_ssem,
    w_rsem,
    a_ssem,
    a_rsem,
    r_ssem,
    r_rsem,
    m_ssem,
    m_rsem,
    d_rsem,
    word_sem,
):
    nz, nx, nc, nt = sizes
    count = nz * nx * nc
    rows = res_v.shape[0]
    width = res_v.shape[1]
    half = width // 2
    cap = pk_send.shape[1] // 2
    tokens = q_v.shape[0]
    tiles = tokens // TILE
    heads = q_v.shape[1] // TILE
    srows = st_send.shape[1] // 2
    per = TILE // srows
    ffp = gu.shape[-1]
    dd = (dd0, dd1, dd2, dd3)
    rt_send = (rts0, rts1, rts2, rts3)
    rt_recv = (rtr0, rtr1, rtr2, rtr3)
    cols = [width * n // 8 for n in EIGHTHS]
    starts = [sum(cols[:j]) for j in range(CHUNKS)]

    z, x, c = (lax.axis_index(a) for a in EP)
    t = lax.axis_index("tp")
    me = (z * nx + x) * nc + c

    def ep_id(p):
        return {
            "ep_0": lax.div(p, nx * nc),
            "ep_1": lax.rem(lax.div(p, nc), nx),
            "ep_2": lax.rem(p, nc),
            "tp": t,
        }

    def y_id(d):
        return {"ep_0": z, "ep_1": x, "ep_2": c, "tp": lax.rem(t + d, nt)}

    def reach(i):
        odd = lax.rem(i, 2)
        return odd * (count // 2 - lax.div(i + 1, 2)) - (1 - odd) * (count // 2 - lax.div(i, 2))

    def peer_of(i):
        return lax.rem(me + reach(i) + count, count)

    def source_of(i):
        return lax.rem(me - reach(i) + count, count)

    t_rows = pl.ds(pl.multiple_of(t * rows, rows), rows)
    pairs = [
        (g_in.at[0], gu.at[0, 0]),
        (u_in.at[0], gu.at[0, 1]),
        (res_in.at[t_rows], res_v),
        (ens_in, ens_v),
        (routes_in, routes_v),
        (mixw_in, mixw_v),
        (q_in, q_v),
        (ff_in, ff_v),
        (fb_in, fb_v),
        (v_in, v_v),
        (og_in, og_v),
        (lbf_in, lbf_v),
        (lbb_in, lbb_v),
        (extra_in, extra_v),
        (hns_in, hns_v),
        (wo_in, wo_v),
    ]
    pairs[2:2] = [
        (d_in.at[0, :, starts[j] : starts[j] + cols[j]], dd[j].at[0:ffp])
        for j in range(CHUNKS)
    ]
    loads = [pltpu.make_async_copy(a, b, ld_sem.at[i]) for i, (a, b) in enumerate(pairs)]
    for copy in loads:
        copy.start()

    def grid_id(dz=0, dx=0, dc=0, dy=0):
        return {
            "ep_0": lax.rem(z + dz, nz),
            "ep_1": lax.rem(x + dx, nx),
            "ep_2": lax.rem(c + dc, nc),
            "tp": lax.rem(t + dy, nt),
        }

    def greet(sem, devices):
        for device in devices:
            pl.semaphore_signal(sem, inc=1, device_id=device, device_id_type=MESH)

    line_y = [grid_id(dy=d) for d in range(1, nt)]
    plane = [grid_id(dx=i, dc=j) for i in range(nx) for j in range(nc) if i + j > 0]
    near_z = [grid_id(dz=d) for d in range(1, nz) if min(d, nz - d) <= (nz + 3) // 4]
    near = line_y + plane + near_z
    barrier = pltpu.get_barrier_semaphore()
    greet(barrier, near)

    for i in range(2 + CHUNKS):
        loads[i].wait()
    pl.semaphore_wait(barrier, len(near))

    def y_copy(k, src, dst, d):
        return pltpu.make_async_remote_copy(
            src_ref=src,
            dst_ref=dst,
            send_sem=w_ssem.at[k],
            recv_sem=w_rsem.at[k],
            device_id=y_id(d),
            device_id_type=MESH,
        )

    g_up = y_copy(0, gu.at[0, 0], gu.at[1, 0], 1)
    u_up = y_copy(1, gu.at[0, 1], gu.at[1, 1], 1)
    u_dn = y_copy(2, gu.at[0, 1], gu.at[2, 1], nt - 1)
    g_dn = y_copy(3, gu.at[0, 0], gu.at[2, 0], nt - 1)
    g_far = y_copy(4, gu.at[1, 0], gu.at[3, 0], 1)
    u_far = y_copy(5, gu.at[2, 1], gu.at[3, 1], nt - 1)
    hh = ffp // 2

    def d_part(s, j, k):
        return dd[j].at[s * ffp + k * hh : s * ffp + (k + 1) * hh]

    def d_copies(j):
        base = 6 + 6 * j
        own = [y_copy(base + k, d_part(0, j, k), d_part(1, j, k), 1) for k in (0, 1)]
        own += [y_copy(base + 2 + k, d_part(0, j, k), d_part(2, j, k), nt - 1) for k in (1, 0)]
        far = [
            y_copy(base + 4, d_part(1, j, 0), d_part(3, j, 0), 1),
            y_copy(base + 5, d_part(2, j, 1), d_part(3, j, 1), nt - 1),
        ]
        return own, far

    d_all = [d_copies(j) for j in range(CHUNKS)]

    for copy in (g_up, u_dn, u_up, g_dn):
        copy.start()
    for copy in d_all[0][0]:
        copy.start()
    greet(word_sem.at[0], near_z)


    for i in range(2 + CHUNKS, 5 + CHUNKS):
        loads[i].wait()
    wide = res_v[...].astype(F32)
    scale = lax.rsqrt(jnp.mean(wide * wide, axis=-1, keepdims=True) + EPS)
    xn[...] = (wide * scale * ens_v[...]).astype(BF16)

    pl.semaphore_wait(word_sem.at[0], len(near_z))
    greet(word_sem.at[1], plane)

    t_lanes = pl.ds(pl.multiple_of(t * rows, rows), rows)
    expert = lax.broadcasted_iota(jnp.int32, (count, rows), 0)
    hit0 = routes_v[0:1, t_lanes] == expert
    hit1 = routes_v[1:2, t_lanes] == expert
    member = jnp.where(hit0, 1.0, 0.0) + jnp.where(hit1, 1.0, 0.0)
    before = lax.broadcasted_iota(jnp.int32, (rows, rows), 0) < lax.broadcasted_iota(
        jnp.int32, (rows, rows), 1
    )
    rank = dot(member.astype(BF16), jnp.where(before, 1.0, 0.0).astype(BF16))
    slot = jnp.where(member > 0.5, rank, -1.0)
    seat = lax.broadcasted_iota(jnp.int32, (count, cap, rows), 1).astype(F32)
    chosen = jnp.where(jnp.abs(slot[:, None, :] - seat) < 0.25, 1.0, 0.0)
    pick[...] = chosen.reshape(count * cap, rows).astype(BF16)

    group = TILE // cap
    parts = count // group

    @pl.loop(0, parts)
    def _(i):
        y = dot(pick[pl.ds(pl.multiple_of(i * TILE, TILE), TILE), :], xn[...])
        lo = y[:, :half].reshape(group, cap, half)
        hi = y[:, half:].reshape(group, cap, half)
        pk_send[pl.ds(i * group, group)] = jnp.concatenate([lo, hi], axis=1).astype(BF16)

    def exchange(src, dst, ssem, rsem):
        @pl.loop(0, count - 1)
        def _(i):
            p = peer_of(i)
            pltpu.make_async_remote_copy(
                src_ref=src.at[p],
                dst_ref=dst.at[me],
                send_sem=ssem,
                recv_sem=rsem,
                device_id=ep_id(p),
                device_id_type=MESH,
            ).start()

    def settle(ref, sem):
        part = ref.at[pl.ds(0, count - 1)]
        pltpu.make_async_copy(part, part, sem).wait()

    pl.semaphore_wait(word_sem.at[1], len(plane))

    def dispatch(k):
        @pl.loop(k * group, min((k + 1) * group, count - 1))
        def _(i):
            p = peer_of(i)
            pltpu.make_async_remote_copy(
                src_ref=pk_send.at[p],
                dst_ref=arr.at[i],
                send_sem=a_ssem.at[0],
                recv_sem=d_rsem.at[k],
                device_id=ep_id(p),
                device_id_type=MESH,
            ).start()

    for k in range(parts // 2):
        dispatch(k)
    arr[count - 1] = pk_send[me]

    for i in range(5 + CHUNKS, len(loads)):
        loads[i].wait()
    row_i = lax.broadcasted_iota(jnp.int32, (TILE, TILE), 0)
    col_i = lax.broadcasted_iota(jnp.int32, (TILE, TILE), 1)
    lower = row_i >= col_i
    upper = row_i <= col_i
    masks = (lower, upper)

    @pl.loop(0, tiles)
    def _(n):
        at = pl.ds(pl.multiple_of(n * TILE, TILE), TILE)
        for h in range(heads):
            ch = slice(h * TILE, (h + 1) * TILE)
            q = q_v[at, ch].astype(F32)
            qf[at, ch] = q * sigmoid(q)
            extra = jnp.broadcast_to(extra_v[h : h + 1, at], (TILE, TILE)).T
            for r, (f_ref, lb_ref) in enumerate(((ff_v, lbf_v), (fb_v, lbb_v))):
                key = sigmoid(-lb_ref[:, ch]) * sigmoid(-f_ref[at, ch].astype(F32))
                small = key * (
                    1.0
                    + key * (0.5 + key * ((1.0 / 3.0) + key * (0.25 + key * 0.2)))
                )
                near = key < 0.03125
                decay = jnp.where(near, -small, jnp.log(jnp.where(near, 0.5, 1.0 - key))) + extra
                tri = jnp.where(masks[r], 1.0, 0.0).astype(BF16)
                first = decay.astype(BF16)
                rest = decay - first.astype(F32)
                second = rest.astype(BF16)
                third = (rest - second.astype(F32)).astype(BF16)
                total = dot(tri, first) + (dot(tri, second) + dot(tri, third))
                p_s[r, at, ch] = total
                k_s[r, at, ch] = key
                last = total[TILE - 1 :, :] if r == 0 else total[:1, :]
                faded = (key * jnp.exp(last - total)).astype(BF16)
                ust[r * heads + h, n] = dot_tn(v_v[at, ch], faded)
                tots[r * heads + h, n] = jnp.broadcast_to(last, (8, TILE))

    for r in range(2):
        for h in range(heads):
            state = jnp.zeros((TILE, TILE), F32)
            log_total = jnp.zeros((1, TILE), F32)
            for n in range(tiles) if r == 0 else reversed(range(tiles)):
                row = tots[r * heads + h, n][:1]
                state = jnp.exp(row) * state + ust[r * heads + h, n]
                log_total = log_total + row
            message = jnp.concatenate(
                [
                    state.reshape(per, srows, TILE),
                    jnp.broadcast_to(log_total[None], (per, srows, TILE)),
                ],
                axis=1,
            )
            st_send[(r * heads + h) * per : (r * heads + h + 1) * per] = message.astype(BF16)

    exchange(st_send, st_recv, a_ssem.at[1], a_rsem.at[1])
    st_recv[me] = st_send[me]
    for k in range(parts // 2, parts):
        dispatch(k)

    @pl.loop(0, tiles)
    def _(n):
        at = pl.ds(pl.multiple_of(n * TILE, TILE), TILE)
        for h in range(heads):
            ch = slice(h * TILE, (h + 1) * TILE)
            q = qf[at, ch]
            scores = None
            for r in range(2):
                total = p_s[r, at, ch]
                key = k_s[r, at, ch]
                blocks = []
                for i in range(TILE // SUB):
                    sub = slice(i * SUB, (i + 1) * SUB)
                    mid = total[i * SUB + SUB // 2 : i * SUB + SUB // 2 + 1, :]
                    q_i = (q[sub] * jnp.exp(total[sub] - mid)).astype(BF16)
                    k_i = (key * jnp.exp(jnp.minimum(mid - total, 70.0))).astype(BF16)
                    blocks.append(dot_nt(q_i, k_i))
                part = jnp.where(masks[r], jnp.concatenate(blocks, axis=0), 0.0)
                scores = part if scores is None else scores + part
            o_s[at, ch] = dot(scores.astype(BF16), v_v[at, ch])

    w0 = mixw_v[0:1, :]
    w1 = mixw_v[1:2, :]
    share = jnp.where(hit0, w0, 0.0) + jnp.where(hit1, w1, 0.0)
    weighted = chosen * share[:, None, :]
    blank = jnp.zeros_like(weighted)
    for k in range(2):
        both = jnp.concatenate([weighted, blank] if k == 0 else [blank, weighted], axis=1)
        flat = both.reshape(count * 2 * cap, rows).T
        high = flat.astype(BF16)
        cwt[0, k * rows : (k + 1) * rows] = high
        cwt[1, k * rows : (k + 1) * rows] = (flat - high.astype(F32)).astype(BF16)

    g_up.wait_recv()
    g_far.start()
    u_dn.wait_recv()
    u_far.start()
    settle(st_recv, a_rsem.at[1])
    side = lax.div(me * srows, heads * TILE)

    def pass_on(i, state):
        g = i + side * (count - 1 - 2 * i)
        inc_send[g] = state
        part = st_recv[g].astype(F32)
        return jnp.exp(part[srows:]) * state + part[:srows]

    lax.fori_loop(0, count, pass_on, jnp.zeros((srows, TILE), F32))
    exchange(inc_send, inc_recv, a_ssem.at[2], a_rsem.at[2])
    inc_recv[me] = inc_send[me]

    def lift(s, lo, size):
        at = pl.ds(pl.multiple_of(lo, TILE), size)
        gated = dot(xs[at, :], gu[s, 0])
        lifted = dot(xs[at, :], gu[s, 1])
        hid[at, s * ffp : (s + 1) * ffp] = (gated * sigmoid(gated) * lifted).astype(BF16)

    def lift_all(s):
        @pl.loop(0, parts // 2)
        def _(i):
            lift(s, i * (2 * TILE), 2 * TILE)

    def unpack(k):
        landed = arr.at[pl.ds(0, min(group, count - 1 - k * group))]
        pltpu.make_async_copy(landed, landed, d_rsem.at[k]).wait()
        block = arr[k * group : (k + 1) * group].astype(F32)
        at = slice(k * TILE, (k + 1) * TILE)
        xs[at, :half] = block[:, :cap].reshape(TILE, half).astype(BF16)
        xs[at, half:] = block[:, cap:].reshape(TILE, half).astype(BF16)
        lift(0, k * TILE, TILE)

    for k in range(parts - 1):
        unpack(k)
    early = (parts - 1) * TILE
    u_up.wait_recv()
    g_dn.wait_recv()
    for n in (1, 2):

        @pl.loop(0, parts - 1)
        def _(i):
            lift(n, i * TILE, TILE)

    unpack(parts - 1)
    for n in (1, 2):
        lift(n, early, TILE)

    d_all[0][0][0].wait_recv()
    d_all[0][1][0].start()
    d_all[0][0][2].wait_recv()
    d_all[0][1][1].start()
    for copy in d_all[1][0]:
        copy.start()

    def finish_recurrence():
        settle(inc_recv, a_rsem.at[2])
        for r in range(2):
            for h in range(heads):
                ch = slice(h * TILE, (h + 1) * TILE)
                k = r * heads + h
                state = inc_recv[k * per : (k + 1) * per].reshape(TILE, TILE)
                for n in range(tiles) if r == 0 else reversed(range(tiles)):
                    at = slice(n * TILE, (n + 1) * TILE)
                    reach = (qf[at, ch] * jnp.exp(p_s[r, at, ch])).astype(BF16)
                    o_s[at, ch] += dot_nt(reach, state.astype(BF16))
                    state = jnp.exp(tots[k, n][:1]) * state + ust[k, n]

        @pl.loop(0, tiles)
        def _(n):
            at = pl.ds(pl.multiple_of(n * TILE, TILE), TILE)
            for h in range(heads):
                ch = slice(h * TILE, (h + 1) * TILE)
                o = o_s[at, ch]
                scaled = (
                    o
                    * lax.rsqrt(jnp.mean(o * o, axis=-1, keepdims=True) + EPS)
                    * hns_v[:, ch]
                )
                gate = og_v[at, ch].astype(F32)
                mh[at, ch] = (scaled * (gate * sigmoid(gate))).astype(BF16)

        @pl.loop(0, nt)
        def _(n):
            at = pl.ds(pl.multiple_of(n * rows, rows), rows)
            mp_send[n] = dot(mh[at, :], wo_v[...]).astype(BF16)

    finish_recurrence()

    g_far.wait_recv()
    u_far.wait_recv()
    lift_all(3)

    def down(j):
        halfc = cols[j] // 2

        def product(i):
            y = dot(hid[pl.ds(pl.multiple_of(i * TILE, TILE), TILE), :], dd[j][...])
            lo = y[:, :halfc].reshape(group, cap, halfc)
            hi = y[:, halfc:].reshape(group, cap, halfc)
            rt_send[j][pl.ds(i * group, group)] = jnp.concatenate([lo, hi], axis=1).astype(BF16)

        def give_back(first, last):
            @pl.loop(first, last)
            def _(i):
                p = source_of(i)
                pltpu.make_async_remote_copy(
                    src_ref=rt_send[j].at[i],
                    dst_ref=rt_recv[j].at[me],
                    send_sem=r_ssem.at[j],
                    recv_sem=r_rsem.at[j],
                    device_id=ep_id(p),
                    device_id_type=MESH,
                ).start()

        product(0)

        @pl.loop(1, parts)
        def _(k):
            product(k)
            give_back((k - 1) * group, k * group)

        give_back((parts - 1) * group, count - 1)
        rt_recv[j][me] = rt_send[j][count - 1]

    hr = rows // 2

    def mixer_copy(k, src, dst, d):
        return pltpu.make_async_remote_copy(
            src_ref=src,
            dst_ref=mp_recv.at[dst],
            send_sem=m_ssem.at[k],
            recv_sem=m_rsem.at[k],
            device_id=y_id(d),
            device_id_type=MESH,
        )

    above, across, below = (lax.rem(t + d, nt) for d in (1, 2, 3))
    mix_first = [
        mixer_copy(0, mp_send.at[across, 0:hr], 0, 1),
        mixer_copy(1, mp_send.at[across, hr:rows], 1, nt - 1),
        mixer_copy(2, mp_send.at[above, hr:rows], 2, 1),
        mixer_copy(3, mp_send.at[below, 0:hr], 3, nt - 1),
    ]
    mix_second = [
        mixer_copy(4, mp_sum.at[0], 4, 1),
        mixer_copy(5, mp_sum.at[1], 5, nt - 1),
    ]

    for j in range(CHUNKS):
        own, far = d_all[j]
        if j > 0:
            own[0].wait_recv()
            far[0].start()
            own[2].wait_recv()
            far[1].start()
            for copy in d_all[j + 1][0] if j + 1 < CHUNKS else mix_first:
                copy.start()
        own[1].wait_recv()
        own[3].wait_recv()
        far[0].wait_recv()
        far[1].wait_recv()
        down(j)

    def combine(j):
        settle(rt_recv[j], r_rsem.at[j])
        halfc = cols[j] // 2
        back = rt_recv[j][...].reshape(count * 2 * cap, halfc)
        y = dot(cwt[0], back) + dot(cwt[1], back)
        routed_out[:, starts[j] : starts[j] + halfc] = y[:rows].astype(BF16)
        routed_out[:, starts[j] + halfc : starts[j] + cols[j]] = y[rows:].astype(BF16)

    mix_first[0].wait_recv()
    mp_sum[0] = (mp_send[above, 0:hr].astype(F32) + mp_recv[0].astype(F32)).astype(BF16)
    mix_second[0].start()
    mix_first[1].wait_recv()
    mp_sum[1] = (mp_send[below, hr:rows].astype(F32) + mp_recv[1].astype(F32)).astype(BF16)
    mix_second[1].start()
    for j in range(CHUNKS - 1):
        combine(j)
    for copy in mix_first[2:] + mix_second:
        copy.wait_recv()
    for k, (one, two) in enumerate(((4, 3), (2, 5))):
        at = slice(k * hr, (k + 1) * hr)
        summed = mp_send[t, at].astype(F32) + mp_recv[one].astype(F32) + mp_recv[two].astype(F32)
        mix_out[at, :] = summed.astype(BF16)
    combine(CHUNKS - 1)

    for copy in (g_up, u_up, u_dn, g_dn, g_far, u_far):
        copy.wait_send()
    for own, far in d_all:
        for copy in own + far:
            copy.wait_send()
    settle(pk_send, a_ssem.at[0])
    settle(st_send, a_ssem.at[1])
    settle(inc_send, a_ssem.at[2])
    for j in range(CHUNKS):
        settle(rt_send[j], r_ssem.at[j])
    for copy in mix_first + mix_second:
        copy.wait_send()


def shards(
    sizes,
    queries,
    forget_forward_logits,
    forget_backward_logits,
    values,
    output_gate_logits,
    lower_bound_forward,
    lower_bound_backward,
    extra_log_decay,
    head_norm_scale,
    output_projection,
    second_residual,
    expert_norm_scale,
    routes,
    specialist_mixing_factor,
    expert_gate_matrix,
    expert_up_matrix,
    expert_down_matrix,
):
    nz, nx, nc, nt = sizes
    count = nz * nx * nc
    tokens, width = second_residual.shape
    rows = tokens // nt
    cap = 4 * rows // count
    chan = queries.shape[1]
    heads = chan // TILE
    tiles = queries.shape[0] // TILE
    srows = 2 * heads * TILE // count
    ffp = expert_gate_matrix.shape[2]
    half = width // 2
    cols = [width * n // 8 for n in EIGHTHS]
    operands = (
        queries,
        forget_forward_logits,
        forget_backward_logits,
        values,
        output_gate_logits,
        lower_bound_forward.reshape(1, chan),
        lower_bound_backward.reshape(1, chan),
        extra_log_decay.T,
        head_norm_scale.reshape(1, chan),
        output_projection,
        second_residual,
        expert_norm_scale.reshape(1, width),
        routes.T,
        specialist_mixing_factor.T,
        expert_gate_matrix,
        expert_up_matrix,
        expert_down_matrix,
    )
    vm = pltpu.VMEM
    scratch = [vm(a.shape, a.dtype) for a in operands[:10]]
    scratch += [vm((rows, width), BF16)]
    scratch += [vm(a.shape, a.dtype) for a in operands[11:14]]
    scratch += [
        vm((4, 2, width, ffp), BF16),
    ]
    scratch += [vm((4 * ffp, n), BF16) for n in cols]
    scratch += [
        vm((rows, width), BF16),
        vm((count * cap, rows), BF16),
        vm((2, 2 * rows, count * 2 * cap), BF16),
        vm((count, 2 * cap, half), BF16),
        vm((count, 2 * cap, half), BF16),
        vm((count * cap, width), BF16),
        vm((count * cap, 4 * ffp), BF16),
    ]
    scratch += [vm((count, 2 * cap, n // 2), BF16) for n in cols + cols]
    scratch += [
        vm((2, tiles * TILE, chan), F32),
        vm((2, tiles * TILE, chan), F32),
        vm((tiles * TILE, chan), F32),
        vm((tiles * TILE, chan), F32),
        vm((2 * heads, tiles, TILE, TILE), F32),
        vm((2 * heads, tiles, 8, TILE), F32),
        vm((count, 2 * srows, TILE), BF16),
        vm((count, 2 * srows, TILE), BF16),
        vm((count, srows, TILE), F32),
        vm((count, srows, TILE), F32),
        vm((tiles * TILE, chan), BF16),
        vm((nt, rows, width), BF16),
        vm((2, rows // 2, width), BF16),
        vm((6, rows // 2, width), BF16),
        pltpu.SemaphoreType.DMA((16 + CHUNKS,)),
        pltpu.SemaphoreType.DMA((6 + 6 * CHUNKS,)),
        pltpu.SemaphoreType.DMA((6 + 6 * CHUNKS,)),
        pltpu.SemaphoreType.DMA((3,)),
        pltpu.SemaphoreType.DMA((3,)),
        pltpu.SemaphoreType.DMA((CHUNKS,)),
        pltpu.SemaphoreType.DMA((CHUNKS,)),
        pltpu.SemaphoreType.DMA((6,)),
        pltpu.SemaphoreType.DMA((6,)),
        pltpu.SemaphoreType.DMA((count * cap // TILE,)),
        pltpu.SemaphoreType.REGULAR((2,)),
    ]
    out = jax.ShapeDtypeStruct((rows, width), BF16)
    return pl.pallas_call(
        functools.partial(kernel, sizes),
        out_shape=(out, out),
        in_specs=[pl.BlockSpec(memory_space=pltpu.HBM)] * len(operands),
        out_specs=(pl.BlockSpec(memory_space=pltpu.VMEM),) * 2,
        scratch_shapes=scratch,
        compiler_params=pltpu.CompilerParams(
            collective_id=0, has_side_effects=True, vmem_limit_bytes=48 * 1024 * 1024
        ),
    )(*(pltpu.with_memory_space_constraint(a, pltpu.HBM) for a in operands))


def solution(mesh):
    tp = mesh.shape["tp"]
    ep = mesh.shape["ep"]
    sizes = (8, 4, 2, tp) if ep == 64 else (ep // 2, 1, 2, tp)
    split = Mesh(mesh.devices.reshape(sizes), EP_TP)
    return jax.shard_map(
        functools.partial(shards, sizes),
        mesh=split,
        in_specs=(
            P(EP, "tp"),
            P(EP, "tp"),
            P(EP, "tp"),
            P(EP, "tp"),
            P(EP, "tp"),
            P("tp"),
            P("tp"),
            P(EP, "tp"),
            P("tp"),
            P("tp", None),
            P(EP, None),
            P(),
            P(EP, None),
            P(EP_TP, None),
            P(EP, None, "tp"),
            P(EP, None, "tp"),
            P(EP, "tp", None),
        ),
        out_specs=(P(EP_TP, None), P(EP_TP, None)),
        check_vma=False,
    )
```
